32 devices in a mesh: sp: 8 (over z, y), tp: 4 (over x, core).
Axes of the slice: x: 2, y: 2, z: 4, core: 2. Of those that a mesh axis runs over, the one named last changes fastest.
Arguments:
- queries: bfloat16 [4096, 1024], P('sp', 'tp'), may hold values from -6 to 6
- keys: bfloat16 [4096, 1024], P('sp', 'tp'), may hold values from -6 to 6
- values: bfloat16 [4096, 1024], P('sp', 'tp'), may hold values from -12 to 12
- breaks: bfloat16 [4096, 8], P('sp', 'tp'), may hold values from -12 to 0.5
- residual_in: bfloat16 [4096, 2048], P('sp', 'tp'), may hold values from -6 to 6
- out_weight: bfloat16 [1024, 2048], P('tp'), may hold values from -0.1875 to 0.1875
- first_gain: float32 [2048], replicated, may hold values from 0.1 to 1.9
- first_shift: float32 [2048], replicated, may hold values from -2 to 2
- up_weight: bfloat16 [2048, 8192], P('sp', 'tp'), may hold values from -0.125 to 0.125
- down_weight: bfloat16 [2048, 8192], P('sp', 'tp'), may hold values from -0.0625 to 0.0625
- second_gain: float32 [2048], replicated, may hold values from 0.1 to 1.9
- second_shift: float32 [2048], replicated, may hold values from -2 to 2
Outputs:
- layer_out: bfloat16 [4096, 2048], P('sp', 'tp')
The draws below stay inside these ranges and needn't reach their ends.
All inputs are finite; a program needn't handle non-finite values.
Results may differ from the reference program's by a relative error of at most 0.018.
Values may be sent and summed in bfloat16 or wider, within the bound.
A program may use at most 128 MiB of HBM per device.

```python
import math
import jax
import jax.numpy as jnp
from jax import lax

D = 2048
FF = 8192
HEAD_COUNT = 8
HD = 128
KEY_BLOCK = 512
TOK_DEV = 512
SEQUENCE_LENGTH = 4096
N_TP = 4


def draw_values(key, part):
    offset_key, noise_key = jax.random.split(jax.random.fold_in(key, 29), 2)
    offset = jax.random.normal(offset_key, (HEAD_COUNT * HD,), jnp.float32) * 1.5
    noise = jax.random.normal(noise_key, (SEQUENCE_LENGTH, HEAD_COUNT * HD), jnp.float32) * 2.0
    return jnp.clip(noise + offset[None, :], -12.0, 12.0).astype(jnp.bfloat16)


def draw_breaks(key, part):
    gradual_key, quick_key, key_tile_rows, noise_key, spike_key, height_key = jax.random.split(jax.random.fold_in(key, 17), 6)
    slow_share = 0.5
    slow_heads = jax.random.uniform(gradual_key, (HEAD_COUNT,)) < slow_share
    slow_base = math.log(1.0 / SEQUENCE_LENGTH) - 0.5
    fast_base = -4.2 + jax.random.uniform(quick_key, (HEAD_COUNT,), minval=-0.3, maxval=0.3)
    head_base = jnp.where(slow_heads, slow_base, fast_base)
    by_block = jax.random.uniform(key_tile_rows, (SEQUENCE_LENGTH // TOK_DEV, HEAD_COUNT), minval=0.0, maxval=math.log(2.5))
    blockwise = jnp.repeat(by_block, TOK_DEV, axis=0)
    jitter = jax.random.uniform(noise_key, (SEQUENCE_LENGTH, HEAD_COUNT), minval=-0.35, maxval=0.35)
    height_values = head_base[None, :] + blockwise + jitter
    spiky_scores = jax.random.uniform(spike_key, (SEQUENCE_LENGTH, HEAD_COUNT)) < 4.0 / SEQUENCE_LENGTH
    spike_height = jax.random.uniform(height_key, (SEQUENCE_LENGTH, HEAD_COUNT), minval=-1.5, maxval=0.0)
    return jnp.where(spiky_scores, spike_height, height_values).astype(jnp.bfloat16)


def block_scale(rng, shape, cuts, least, high):
    level = 1.0
    for dim, parts in cuts:
        heights = jax.random.uniform(jax.random.fold_in(jax.random.fold_in(rng, 6), dim), (parts,), jnp.float32, least / len(cuts), high / len(cuts))
        level = level * jnp.repeat(jnp.exp(heights), shape[dim] // parts).reshape((-1,) + (1,) * (len(shape) - 1 - dim))
    return level


def scatter_about(own_key, extent, width, limit, cuts=(), kind=jnp.bfloat16):
    factor_of = block_scale(own_key, extent, cuts, -0.22, 0.18) if cuts else 1.0
    drawn = jax.random.normal(own_key, extent, jnp.float32) * width * factor_of
    return jnp.minimum(jnp.maximum(drawn, -limit), limit).astype(kind)


def setup_inputs(seed: int = 0) -> dict:
    seeds = jax.random.split(jax.random.key(seed), 13)
    queries = scatter_about(seeds[0], (SEQUENCE_LENGTH, HEAD_COUNT * HD), 1.0, 6.0, ((0, 8), (1, 4)))
    keys = scatter_about(seeds[1], (SEQUENCE_LENGTH, HEAD_COUNT * HD), 1.0, 6.0, ((0, 8), (1, 4)))
    values = draw_values(jax.random.fold_in(seeds[12], 71), 0)
    breaks = draw_breaks(jax.random.fold_in(seeds[12], 71), 0)
    residual_in = scatter_about(seeds[4], (SEQUENCE_LENGTH, D), 1.0, 6.0, ((0, 8), (1, 4)))
    out_weight = scatter_about(seeds[5], (HEAD_COUNT * HD, D), (HEAD_COUNT * HD) ** -0.5, 0.1875, ((0, 4),))
    first_gain = jnp.clip(1.0 + 0.18 * jax.random.normal(seeds[6], (D,), jnp.float32), 0.1, 1.9)
    first_shift = scatter_about(seeds[7], (D,), 0.3, 2.0, (), jnp.float32)
    up_weight = scatter_about(seeds[8], (D, FF), D ** -0.5, 0.125, ((0, 8), (1, 4)))
    down_weight = scatter_about(seeds[9], (D, FF), FF ** -0.5, 0.0625, ((0, 8), (1, 4)))
    second_gain = jnp.clip(1.0 + 0.18 * jax.random.normal(seeds[10], (D,), jnp.float32), 0.1, 1.9)
    second_shift = scatter_about(seeds[11], (D,), 0.3, 2.0, (), jnp.float32)
    return dict(queries=queries, keys=keys, values=values, breaks=breaks, residual_in=residual_in, out_weight=out_weight, first_gain=first_gain, first_shift=first_shift, up_weight=up_weight, down_weight=down_weight, second_gain=second_gain, second_shift=second_shift)


ALPHA = 2.0 ** 0.25
EPSILON = 1e-05

def rounded(partial_value):
    return lax.optimization_barrier(partial_value.astype(jnp.bfloat16)).astype(jnp.float32)

def layer_norm(pre, gain, shift):
    center = lax.optimization_barrier(jnp.mean(pre, axis=-1, keepdims=True))
    centered = pre - center
    spread = lax.optimization_barrier(jnp.mean(centered * centered, axis=-1, keepdims=True))
    return centered * lax.rsqrt(spread + EPSILON) * gain + shift

def reference(queries, keys, values, breaks, residual_in, out_weight, first_gain, first_shift, up_weight, down_weight, second_gain, second_shift):
    query_heads = queries.reshape(SEQUENCE_LENGTH, HEAD_COUNT, HD).astype(jnp.float32)
    key_heads = keys.reshape(SEQUENCE_LENGTH, HEAD_COUNT, HD).astype(jnp.float32)
    value_heads = values.reshape(SEQUENCE_LENGTH, HEAD_COUNT, HD).astype(jnp.float32)
    break_rows = breaks.astype(jnp.float32).T
    positions = jnp.arange(SEQUENCE_LENGTH, dtype=jnp.int32)
    scale = HD ** (-0.5)

    def attend_block(index):
        first = index * KEY_BLOCK
        query_block = lax.dynamic_slice_in_dim(query_heads, first, KEY_BLOCK, 0)
        query_pos = first + jnp.arange(KEY_BLOCK, dtype=jnp.int32)
        scores = jnp.einsum('qhd,khd->hqk', query_block, key_heads) * scale + break_rows[:, None, :]
        strict = (positions[None, :] < query_pos[:, None])[None]
        log_break = jax.nn.log_sigmoid(scores)
        log_keep = jnp.where(strict, log_break - scores, 0.0)
        later = lax.cumsum(log_keep, axis=2, reverse=True) - log_keep
        weights = jnp.where(strict, jnp.exp(log_break + later), 0.0).astype(jnp.bfloat16)
        mixed_heads = jnp.einsum('hqk,khd->qhd', weights.astype(jnp.float32), value_heads)
        return mixed_heads.reshape(KEY_BLOCK, HEAD_COUNT * HD).astype(jnp.bfloat16)
    attended = lax.map(attend_block, jnp.arange(SEQUENCE_LENGTH // KEY_BLOCK, dtype=jnp.int32)).reshape(SEQUENCE_LENGTH, HEAD_COUNT * HD)
    group_width = HEAD_COUNT * HD // N_TP
    attended_groups = attended.reshape(SEQUENCE_LENGTH, N_TP, group_width).transpose(1, 0, 2)
    out_groups = out_weight.reshape(N_TP, group_width, D)

    def add_group(total, pair):
        return (total + rounded(jnp.dot(pair[0], pair[1], preferred_element_type=jnp.float32)), None)
    mixed = lax.scan(add_group, jnp.zeros((SEQUENCE_LENGTH, D), jnp.float32), (attended_groups, out_groups))[0]
    first_out = layer_norm(ALPHA * residual_in.astype(jnp.float32) + mixed, first_gain, first_shift).astype(jnp.bfloat16)
    hidden_width = FF // N_TP
    up_groups = up_weight.reshape(D, N_TP, hidden_width).transpose(1, 0, 2)
    down_groups = down_weight.reshape(D, N_TP, hidden_width).transpose(1, 0, 2)

    def add_hidden(total, pair):
        activated = jnp.square(jax.nn.relu(jnp.dot(first_out, pair[0], preferred_element_type=jnp.float32))).astype(jnp.bfloat16)
        partial_value = lax.dot_general(activated, pair[1], (((1,), (1,)), ((), ())), preferred_element_type=jnp.float32)
        return (total + rounded(partial_value), None)
    channel_mix = lax.scan(add_hidden, jnp.zeros((SEQUENCE_LENGTH, D), jnp.float32), (up_groups, down_groups))[0]
    second = layer_norm(ALPHA * first_out.astype(jnp.float32) + channel_mix, second_gain, second_shift)
    return second.astype(jnp.bfloat16)
```

```python
import functools

import jax
import jax.numpy as jnp
from jax import lax
from jax.experimental import pallas as pl
from jax.experimental.pallas import tpu as pltpu
from jax.sharding import PartitionSpec as P

ALPHA = 2.0**0.25
EPSILON = 1e-05
MESH = pl.DeviceIdType.MESH
F32 = jnp.float32
BF16 = jnp.bfloat16
KV, UP, DOWN = 0, 1, 2
RIGHT, LEFT = 0, 1


def aligned(start, size):
    return pl.ds(pl.multiple_of(start, size), size)


def layer_kernel(
    n,
    t,
    heads,
    q_ref,
    kv_in,
    br_in,
    res_in,
    ow_in,
    g1_ref,
    b1_ref,
    up_in,
    down_in,
    g2_ref,
    b2_ref,
    out_ref,
    kv,
    up,
    down,
    br,
    ow,
    res,
    later_sum,
    totals,
    att_all,
    lower,
    pre,
    first,
    activated,
    part,
    mix,
    stat,
    ring_send,
    ring_recv,
    br_send,
    br_recv,
    ow_send,
    ow_recv,
    res_send,
    res_recv,
    att_send,
    att_recv,
    mix_send,
    mix_recv,
    stat_send,
    stat_recv,
    local_sem,
):
    me = lax.axis_index("sp")
    me_t = lax.axis_index("tp")
    tok = q_ref.shape[0]
    width = q_ref.shape[1]
    hd = width // heads
    feat = first.shape[1]
    cols = feat // t
    block = feat // n
    per = n // t
    half_n = n // 2

    def at_pos(p):
        p = lax.rem(p + n, n)
        back = p // half_n
        return 2 * (p + back * (n - 1 - 2 * p)) + back

    pos = me // 2 + lax.rem(me, 2) * (n - 1 - 2 * (me // 2))
    next_dev = (at_pos(pos + 1), at_pos(pos - 1))
    own_in = (kv_in, up_in, down_in)
    full = (kv, up, down)
    rows_of = (tok, block, block)

    def ring_copy(item, way, hop, piece, own=False):
        rows = rows_of[item]
        half = rows // 2
        owner = at_pos(pos - (hop - 1) if way == RIGHT else pos + (hop - 1))
        dst = full[item].at[aligned(owner * rows + piece * half, half)]
        src = own_in[item].at[aligned(piece * half, half)] if own else dst
        return pltpu.make_async_remote_copy(
            src_ref=src,
            dst_ref=dst,
            send_sem=ring_send.at[item, way, hop, piece],
            recv_sem=ring_recv.at[item, way, hop, piece],
            device_id={"sp": next_dev[way]},
            device_id_type=MESH,
        )

    def ring_landed(item, way, hop, piece):
        rows = rows_of[item]
        half = rows // 2
        owner = at_pos(pos - hop if way == RIGHT else pos + hop)
        dst = full[item].at[aligned(owner * rows + piece * half, half)]
        return pltpu.make_async_remote_copy(
            src_ref=dst,
            dst_ref=dst,
            send_sem=ring_send.at[item, way, hop, piece],
            recv_sem=ring_recv.at[item, way, hop, piece],
            device_id={"sp": next_dev[way]},
            device_id_type=MESH,
        )

    def start_own(item):
        ring_copy(item, RIGHT, 1, 0, own=True).start()
        ring_copy(item, LEFT, 1, 1, own=True).start()
        ring_copy(item, RIGHT, 1, 1, own=True).start()
        ring_copy(item, LEFT, 1, 0, own=True).start()

    def event(item, e, hop=None, second=None):
        static = isinstance(e, int)
        hop = 1 + e // 2
        second = e % 2 if static else lax.rem(e, 2)
        ring_landed(item, RIGHT, hop, second).wait_recv()

        def forward_right():
            ring_copy(item, RIGHT, hop + 1, second).start()

        def forward_left():
            ring_copy(item, LEFT, hop + 1, 1 - second).start()

        def start_next():
            if item < DOWN:
                start_own(item + 1)

        def guarded(cond, fn):
            if static:
                if cond:
                    fn()
            else:
                pl.when(cond)(fn)

        guarded(e < n - 3, forward_right)
        ring_landed(item, LEFT, hop, 1 - second).wait_recv()
        guarded(e < n - 3, forward_left)
        guarded(e == n - 4, start_next)

    def drain_sends(item):
        def one(e, _):
            hop = 1 + e // 2
            second = lax.rem(e, 2)
            ring_copy(item, RIGHT, hop, second).wait_send()
            ring_copy(item, LEFT, hop, 1 - second).wait_send()
            return 0

        lax.fori_loop(0, n - 1, one, 0)

    def peer_t(d):
        return lax.rem(me_t + d, t)

    def tp_copy(src, dst_of, sends, recvs, d):
        return pltpu.make_async_remote_copy(
            src_ref=src,
            dst_ref=dst_of(me_t),
            send_sem=sends.at[d],
            recv_sem=recvs.at[d],
            device_id={"tp": peer_t(d)},
            device_id_type=MESH,
        )

    def tp_landed(dst_of, sends, recvs, d):
        dst = dst_of(lax.rem(me_t + t - d, t))
        return pltpu.make_async_remote_copy(
            src_ref=dst,
            dst_ref=dst,
            send_sem=sends.at[d],
            recv_sem=recvs.at[d],
            device_id={"tp": peer_t(d)},
            device_id_type=MESH,
        )

    def br_copy(d, landed=False):
        owner = lax.rem(me + n - d, n) if landed else me
        return pltpu.make_async_remote_copy(
            src_ref=br.at[owner] if landed else br_in,
            dst_ref=br.at[owner],
            send_sem=br_send.at[d],
            recv_sem=br_recv.at[d],
            device_id={"sp": lax.rem(me + d, n)},
            device_id_type=MESH,
        )

    barrier = pltpu.get_barrier_semaphore()

    def greet(d, _):
        pl.semaphore_signal(
            barrier, inc=1, device_id={"sp": lax.rem(me + d, n)}, device_id_type=MESH
        )
        return 0

    lax.fori_loop(1, n, greet, 0)
    for d in range(1, t):
        pl.semaphore_signal(barrier, inc=1, device_id={"tp": peer_t(d)}, device_id_type=MESH)

    res_at = lambda g: res.at[g]
    ow_at = lambda g: ow.at[g]
    att_at = lambda g: att_all.at[g]

    locals_ = [
        pltpu.make_async_copy(kv_in, kv.at[aligned(me * tok, tok)], local_sem.at[0]),
        pltpu.make_async_copy(up_in, up.at[aligned(me * block, block)], local_sem.at[1]),
        pltpu.make_async_copy(down_in, down.at[aligned(me * block, block)], local_sem.at[2]),
        pltpu.make_async_copy(br_in, br.at[me], local_sem.at[3]),
        pltpu.make_async_copy(res_in, res.at[me_t], local_sem.at[4]),
        pltpu.make_async_copy(ow_in, ow.at[me_t], local_sem.at[5]),
    ]
    pl.semaphore_wait(barrier, n - 1 + t - 1)
    start_own(KV)

    def send_breaks(d, _):
        br_copy(d).start()
        return 0

    lax.fori_loop(1, n, send_breaks, 0)
    for c in locals_:
        c.start()
    for d in range(1, t):
        tp_copy(ow_in, ow_at, ow_send, ow_recv, d).start()
    for d in range(1, t):
        tp_copy(res_in, res_at, res_send, res_recv, d).start()

    key_row = lax.broadcasted_iota(jnp.int32, (tok, tok), 0)
    key_col = lax.broadcasted_iota(jnp.int32, (tok, tok), 1)
    lower[...] = jnp.where(key_row > key_col, 1.0, 0.0).astype(BF16)
    later_sum[...] = jnp.zeros_like(later_sum)
    totals[...] = jnp.zeros_like(totals)

    def kv_event(e, _):
        event(KV, e)
        return 0

    lax.fori_loop(0, n - 2, kv_event, 0)

    def last_event(item):
        ring_landed(item, RIGHT, half_n, 0).wait_recv()
        ring_landed(item, LEFT, half_n, 1).wait_recv()

    last_event(KV)

    def wait_breaks(d, _):
        br_copy(d, landed=True).wait_recv()
        return 0

    lax.fori_loop(1, n, wait_breaks, 0)
    for c in locals_:
        c.wait()

    scale = hd ** (-0.5)
    tile = 128

    def attend_block(j):
        b = me - j
        for h in range(heads):
            def rows(i, _):
                at = aligned(i * tile, tile)
                keys = kv[aligned(b * tok, tok), pl.ds(h * hd, hd)]
                vals = kv[aligned(b * tok, tok), pl.ds(width + h * hd, hd)]
                z = lax.dot_general(
                    q_ref[at, pl.ds(h * hd, hd)],
                    keys,
                    (((1,), (1,)), ((), ())),
                    preferred_element_type=F32,
                )
                z = z * scale + br[b, pl.ds(h, 1), :]
                soft = jnp.log(1.0 + jnp.exp(-jnp.abs(z)))
                log_break = jnp.minimum(z, 0.0) - soft
                r = lax.broadcasted_iota(jnp.int32, (tile, tok), 0) + i * tile + j * tok
                strict = lax.broadcasted_iota(jnp.int32, (tile, tok), 1) < r
                log_keep = jnp.where(strict, log_break - z, 0.0)
                high = log_keep.astype(BF16)
                low = (log_keep - high.astype(F32)).astype(BF16)
                tri = lower[...]
                later = jnp.dot(high, tri, preferred_element_type=F32) + jnp.dot(
                    low, tri, preferred_element_type=F32
                )
                before = later_sum[h, at, :]
                w = jnp.exp(log_break + later + before[:, 0:1])
                w = jnp.where(strict, w, 0.0).astype(BF16)
                totals[at, pl.ds(h * hd, hd)] += jnp.dot(w, vals, preferred_element_type=F32)
                later_sum[h, at, :] = before + jnp.sum(log_keep, axis=1, keepdims=True)
                return 0

            lax.fori_loop(0, tok // tile, rows, 0)

    def attend_step(j, _):
        @pl.when(j <= me)
        def _():
            attend_block(j)

        @pl.when(j < n - 2)
        def _():
            event(UP, j)

        return 0

    lax.fori_loop(0, n, attend_step, 0)

    own_att = att_all.at[me_t]
    own_att[...] = totals[...].astype(BF16)
    for d in range(1, t):
        tp_copy(own_att, att_at, att_send, att_recv, d).start()
    last_event(UP)
    for d in range(1, t):
        tp_landed(ow_at, ow_send, ow_recv, d).wait_recv()
        tp_landed(res_at, res_send, res_recv, d).wait_recv()
    for d in range(1, t):
        tp_landed(att_at, att_send, att_recv, d).wait_recv()

    big = 256

    def mix_rows(i, _):
        at = aligned(i * big, big)
        for c in range(t):
            lanes = pl.ds(c * cols, cols)
            acc = ALPHA * res[c, at, :].astype(F32)
            mixed = jnp.zeros((big, cols), F32)
            for g in range(t):
                mixed = mixed + jnp.dot(
                    att_all[g, at, :], ow[g, :, lanes], preferred_element_type=F32
                ).astype(BF16).astype(F32)
            pre[at, lanes] = acc + mixed
        return 0

    lax.fori_loop(0, tok // big, mix_rows, 0)
    event(DOWN, 0)

    small = 64

    def norm_rows(i, _):
        at = aligned(i * small, small)
        x = pre[at, :]
        center = jnp.sum(x, axis=1, keepdims=True) / feat
        x = x - center
        spread = jnp.sum(x * x, axis=1, keepdims=True) / feat
        first[at, :] = (x * lax.rsqrt(spread + EPSILON) * g1_ref[...] + b1_ref[...]).astype(BF16)
        return 0

    lax.fori_loop(0, tok // small, norm_rows, 0)

    hidden = up.shape[1]
    strip = 256

    def up_cols(i, _):
        lanes = aligned(i * strip, strip)
        a = jnp.dot(first[...], up[:, lanes], preferred_element_type=F32)
        a = jnp.maximum(a, 0.0)
        activated[:, lanes] = (a * a).astype(BF16)
        return 0

    event(DOWN, 1)
    lax.fori_loop(0, hidden // strip, up_cols, 0)

    def mix_copy(s):
        k = lax.rem(s, per)
        owner = s // per
        return owner, pltpu.make_async_remote_copy(
            src_ref=part.at[s],
            dst_ref=mix.at[me_t, k],
            send_sem=mix_send.at[s],
            recv_sem=mix_recv.at[me_t, k],
            device_id={"tp": owner},
            device_id_type=MESH,
        )

    def down_block(s):
        y = lax.dot_general(
            activated[...],
            down[aligned(s * block, block), :],
            (((1,), (1,)), ((), ())),
            preferred_element_type=F32,
        ).astype(BF16)
        owner, copy = mix_copy(s)

        @pl.when(owner == me_t)
        def _():
            mix[me_t, lax.rem(s, per)] = y

        @pl.when(owner != me_t)
        def _():
            part[s] = y
            copy.start()

    down_block(me)

    def down_step(h, _):
        @pl.when(h > 1)
        def _():
            event(DOWN, 2 * h - 2)
            event(DOWN, 2 * h - 1)

        def side(w, _):
            down_block(at_pos(pos + (2 * w - 1) * h))
            return 0

        lax.fori_loop(0, 2, side, 0)
        return 0

    lax.fori_loop(1, half_n, down_step, 0)
    last_event(DOWN)
    down_block(at_pos(pos + half_n))

    def mix_wait(s, _):
        owner, copy = mix_copy(s)

        @pl.when(owner != me_t)
        def _():
            copy.wait_send()

        return 0

    for d in range(1, t):
        g = lax.rem(me_t + t - d, t)
        for k in range(per):
            dst = mix.at[g, k]
            pltpu.make_async_remote_copy(
                src_ref=dst,
                dst_ref=dst,
                send_sem=mix_send.at[0],
                recv_sem=mix_recv.at[g, k],
                device_id={"tp": peer_t(d)},
                device_id_type=MESH,
            ).wait_recv()

    def second_pre(i, _):
        at = aligned(i * 128, 128)
        sums = jnp.zeros((128, 1), F32)
        squares = jnp.zeros((128, 1), F32)
        x = ALPHA * first[at, aligned(me_t * cols, cols)].astype(F32)
        pieces = []
        for k in range(per):
            v = mix[0, k, at, :].astype(F32)
            for g in range(1, t):
                v = v + mix[g, k, at, :].astype(F32)
            pieces.append(v)
        x = x + (jnp.concatenate(pieces, axis=1) if per > 1 else pieces[0])
        pre[at, pl.ds(0, cols)] = x
        sums = jnp.sum(x, axis=1, keepdims=True)
        squares = jnp.sum(x * x, axis=1, keepdims=True)
        lane = lax.broadcasted_iota(jnp.int32, (128, 128), 1)
        s = jnp.where(lane == 0, sums, jnp.where(lane == 1, squares, 0.0))
        stat[me_t, :, at] = s.T[0:8, :]
        return 0

    for i in range(tok // 128):
        second_pre(i, 0)
    stat_at = lambda g: stat.at[g]
    for d in range(1, t):
        tp_copy(stat.at[me_t], stat_at, stat_send, stat_recv, d).start()

    lax.fori_loop(0, n, mix_wait, 0)
    for item in (KV, UP, DOWN):
        drain_sends(item)

    def br_done(d, _):
        br_copy(d).wait_send()
        return 0

    lax.fori_loop(1, n, br_done, 0)
    for d in range(1, t):
        tp_copy(ow_in, ow_at, ow_send, ow_recv, d).wait_send()
        tp_copy(res_in, res_at, res_send, res_recv, d).wait_send()
        tp_copy(own_att, att_at, att_send, att_recv, d).wait_send()
    for d in range(1, t):
        tp_landed(stat_at, stat_send, stat_recv, d).wait_recv()

    for i in range(tok // 128):
        at = pl.ds(i * 128, 128)
        s = stat[0, :, at]
        for g in range(1, t):
            s = s + stat[g, :, at]
        s = jnp.concatenate([s, jnp.zeros((120, 128), F32)], axis=0).T
        center = s[:, 0:1] / feat
        spread = s[:, 1:2] / feat - center * center
        x = pre[at, pl.ds(0, cols)]
        x = (x - center) * lax.rsqrt(spread + EPSILON)
        out_ref[at, :] = (x * g2_ref[me_t] + b2_ref[me_t]).astype(BF16)
    for d in range(1, t):
        tp_copy(stat.at[me_t], stat_at, stat_send, stat_recv, d).wait_send()


GROUP = 4


def flip(a, r):
    bit = 1
    out = a
    while bit <= r:
        if r & bit:
            out = out + bit - 2 * bit * lax.rem(a // bit, 2)
        bit *= 2
    return out


def remote(src, dst, send, recv, **where):
    return pltpu.make_async_remote_copy(
        src_ref=src,
        dst_ref=dst,
        send_sem=send,
        recv_sem=recv,
        device_id=where,
        device_id_type=MESH,
    )


def grouped_kernel(
    n,
    t,
    q_in,
    k_in,
    v_in,
    br_in,
    res_in,
    ow_in,
    g1_ref,
    b1_ref,
    up_in,
    down_in,
    g2_ref,
    b2_ref,
    out_ref,
    kvb,
    qb,
    br,
    later_sum,
    totals,
    att_own,
    att_all,
    tri_ref,
    ow,
    res,
    pre,
    first,
    up,
    down,
    act,
    pair_out,
    pair_in,
    summed,
    near_in,
    cross_out,
    cross_in,
    mixed_ref,
    stat,
    kv_send,
    kv_recv,
    kx_send,
    kx_recv,
    br_send,
    br_recv,
    ow_send,
    ow_recv,
    res_send,
    res_recv,
    att_send,
    att_recv,
    w_send,
    w_recv,
    t1_send,
    t1_recv,
    t2_send,
    t2_recv,
    t3_send,
    t3_recv,
    pair_send,
    pair_recv,
    near_send,
    near_recv,
    cross_send,
    cross_recv,
    stat_send,
    stat_recv,
    local_sem,
    go_sem,
):
    s = lax.axis_index("sp")
    q = lax.axis_index("tp")
    y = lax.rem(s, 2)
    z = s // 2
    levels = n // 2
    m = lax.rem(s, GROUP)
    group = s // GROUP
    x = q // 2
    c = lax.rem(q, 2)
    tok, width = q_in.shape
    hd = width // 2
    feat = ow.shape[2]
    cols = feat // t
    half_feat = feat // 2
    block = up_in.shape[0]
    sub = up_in.shape[1] // GROUP
    part = tok // 2
    half_n = n // 2
    sibling = flip(q, 1)
    across = flip(q, 2)

    barrier = pltpu.get_barrier_semaphore()
    for r in range(1, n):
        pl.semaphore_signal(barrier, inc=1, device_id={"sp": flip(s, r)}, device_id_type=MESH)
    for r in range(1, t):
        pl.semaphore_signal(barrier, inc=1, device_id={"tp": flip(q, r)}, device_id_type=MESH)
        pl.semaphore_signal(
            barrier, inc=1, device_id={"sp": flip(s, 1), "tp": flip(q, r)}, device_id_type=MESH
        )

    def lanes_of(i, size):
        return aligned(i * size, size)

    own_copies = [
        pltpu.make_async_copy(
            k_in.at[:, lanes_of(y, hd)], kvb.at[s, :, pl.ds(0, hd)], local_sem.at[0]
        ),
        pltpu.make_async_copy(
            v_in.at[:, lanes_of(y, hd)], kvb.at[s, :, pl.ds(hd, hd)], local_sem.at[1]
        ),
        pltpu.make_async_copy(q_in.at[:, lanes_of(y, hd)], qb.at[y], local_sem.at[2]),
    ]
    other_copies = [
        pltpu.make_async_copy(br_in, br.at[s], local_sem.at[3]),
        pltpu.make_async_copy(res_in.at[lanes_of(c, part)], res.at[q], local_sem.at[4]),
        pltpu.make_async_copy(ow_in, ow.at[q], local_sem.at[5]),
        pltpu.make_async_copy(
            up_in.at[:, lanes_of(m, sub)], up.at[lanes_of(s, block)], local_sem.at[6]
        ),
        pltpu.make_async_copy(
            down_in.at[:, lanes_of(m, sub)], down.at[lanes_of(s, block)], local_sem.at[7]
        ),
    ]
    for cp in own_copies:
        cp.start()

    ps = flip(s, 1)
    py = 1 - y

    def exchange(landed=False):
        own = ps if landed else s
        row = y if landed else py
        mine = py if landed else y
        return [
            remote(
                kvb.at[own, :, pl.ds(0, hd)] if landed else k_in.at[:, lanes_of(row, hd)],
                kvb.at[own, :, pl.ds(0, hd)],
                kx_send.at[0],
                kx_recv.at[0],
                sp=ps,
            ),
            remote(
                kvb.at[own, :, pl.ds(hd, hd)] if landed else v_in.at[:, lanes_of(row, hd)],
                kvb.at[own, :, pl.ds(hd, hd)],
                kx_send.at[1],
                kx_recv.at[1],
                sp=ps,
            ),
            remote(
                qb.at[mine] if landed else q_in.at[:, lanes_of(row, hd)],
                qb.at[mine],
                kx_send.at[2],
                kx_recv.at[2],
                sp=ps,
            ),
        ]

    def relay(slot):
        return remote(kvb.at[slot], kvb.at[slot], kv_send.at[slot], kv_recv.at[slot], sp=s + 2)

    def relay_landed(slot):
        return remote(kvb.at[slot], kvb.at[slot], kv_send.at[slot], kv_recv.at[slot], sp=s)

    def br_copy(r, landed=False):
        owner = flip(s, r) if landed else s
        return remote(
            br.at[owner] if landed else br_in,
            br.at[owner],
            br_send.at[r],
            br_recv.at[r],
            sp=flip(s, r),
        )

    def ow_copy(r, landed=False):
        owner = flip(q, r) if landed else q
        return remote(
            ow.at[owner] if landed else ow_in,
            ow.at[owner],
            ow_send.at[r],
            ow_recv.at[r],
            tp=flip(q, r),
        )

    def res_copy(r, landed=False):
        to = flip(q, r)
        owner = to if landed else q
        return remote(
            res.at[owner] if landed else res_in.at[lanes_of(lax.rem(to, 2), part)],
            res.at[owner],
            res_send.at[r],
            res_recv.at[r],
            tp=to,
        )

    mats_in = (up_in, down_in)
    mats = (up, down)

    def w_copy(mat, r, landed=False):
        to = flip(s, r)
        owner = to if landed else s
        dst = mats[mat].at[lanes_of(owner, block)]
        return remote(
            dst if landed else mats_in[mat].at[:, lanes_of(lax.rem(to, GROUP), sub)],
            dst,
            w_send.at[mat, r],
            w_recv.at[mat, r],
            sp=to,
        )

    order = [r for r in range(n - 1, 0, -1)]

    def climbs(r):
        top = 1
        while top * 2 <= r:
            top *= 2
        if top < 2:
            return None
        return lax.rem(s // top, 2) == 0

    def send_mat(mat, upward):
        for r in order:
            up_cond = climbs(r)

            def go(r=r):
                w_copy(mat, r).start()

            if up_cond is None:
                if not upward:
                    go()
            else:
                pl.when(up_cond if upward else jnp.logical_not(up_cond))(go)

    pl.semaphore_wait(barrier, n - 1 + 2 * (t - 1))
    for cp in exchange():
        cp.start()
    for r in range(1, n):
        br_copy(r).start()
    for cp in other_copies:
        cp.start()
    for cp in own_copies:
        cp.wait()

    @pl.when(z < levels - 1)
    def _():
        relay(s).start()

    for r in range(1, t):
        ow_copy(r).start()
    for r in range(1, t):
        res_copy(r).start()
    send_mat(0, False)

    key_row = lax.broadcasted_iota(jnp.int32, tri_ref.shape, 0)
    key_col = lax.broadcasted_iota(jnp.int32, tri_ref.shape, 1)
    tri_ref[...] = jnp.where(key_row > key_col, 1.0, 0.0).astype(BF16)
    later_sum[...] = jnp.zeros_like(later_sum)
    totals[...] = jnp.zeros_like(totals)

    for cp in exchange(landed=True):
        cp.wait_recv()

    @pl.when(z < levels - 1)
    def _():
        relay(ps).start()

    for r in range(1, n):
        br_copy(r, landed=True).wait_recv()
    for cp in other_copies:
        cp.wait()

    scale = hd ** (-0.5)
    tile = 128
    span = tri_ref.shape[0]

    def attend(slot, qy, masked):
        def rows(i, _):
            at = aligned(i * tile, tile)
            z_ = lax.dot_general(
                qb[qy, at, :],
                kvb[slot, :, pl.ds(0, hd)],
                (((1,), (1,)), ((), ())),
                preferred_element_type=F32,
            )
            z_ = z_ * scale + br[slot, pl.ds(y, 1), :]
            soft = jnp.log(1.0 + jnp.exp(-jnp.abs(z_)))
            log_break = jnp.minimum(z_, 0.0) - soft
            keep = log_break - z_
            if masked:
                r = lax.broadcasted_iota(jnp.int32, (tile, tok), 0) + i * tile
                strict = lax.broadcasted_iota(jnp.int32, (tile, tok), 1) < r
                keep = jnp.where(strict, keep, 0.0)
            high = keep.astype(BF16)
            low = (keep - high.astype(F32)).astype(BF16)
            tri = tri_ref[...]
            run = later_sum[qy, at, :][:, 0:1]
            pieces = []
            for b in range(tok // span - 1, -1, -1):
                sl = slice(b * span, (b + 1) * span)
                later = jnp.dot(high[:, sl], tri, preferred_element_type=F32) + jnp.dot(
                    low[:, sl], tri, preferred_element_type=F32
                )
                pieces.append(later + run)
                run = run + jnp.sum(keep[:, sl], axis=1, keepdims=True)
            w = jnp.exp(log_break + jnp.concatenate(pieces[::-1], axis=1))
            if masked:
                w = jnp.where(strict, w, 0.0)
            totals[qy, at, :] += jnp.dot(
                w.astype(BF16), kvb[slot, :, pl.ds(hd, hd)], preferred_element_type=F32
            )
            later_sum[qy, at, :] = jnp.broadcast_to(run, (tile, 128))
            return 0

        lax.fori_loop(0, tok // tile, rows, 0)

    attend(2 * z + 1, 1, True)
    attend(2 * z, 0, True)
    attend(2 * z, 1, False)

    def attend_step(k, _):
        slot = 2 * z + 1 - k

        @pl.when(slot >= 0)
        def _():
            relay_landed(slot).wait_recv()

            @pl.when(z < levels - 1)
            def _():
                relay(slot).start()

            def one(qy, _):
                attend(slot, qy, False)
                return 0

            lax.fori_loop(0, 2, one, 0)

        return 0

    lax.fori_loop(2, n, attend_step, 0)

    @pl.when(z == 1)
    def _():
        pl.semaphore_signal(go_sem, inc=1, device_id={"sp": s - 2}, device_id_type=MESH)

    @pl.when(z == 0)
    def _():
        pl.semaphore_wait(go_sem, 1)

    send_mat(0, True)

    att_own[...] = totals[...].astype(BF16)
    att_list = [(dy, r) for dy in range(2) for r in range(t) if dy or r]

    def att_copy(i, landed=False):
        dy, r = att_list[i]
        ty = flip(y, 1) if dy else y
        tq = flip(q, r)
        sp = ps if dy else s
        if landed:
            dst = att_all.at[tq, :, lanes_of(ty, hd)]
            return remote(dst, dst, att_send.at[i], att_recv.at[i], sp=sp, tp=tq)
        return remote(
            att_own.at[ty, lanes_of(lax.rem(tq, 2), part)],
            att_all.at[q, :, lanes_of(y, hd)],
            att_send.at[i],
            att_recv.at[i],
            sp=sp,
            tp=tq,
        )

    for i in range(len(att_list)):
        att_copy(i).start()
    att_all[q, :, lanes_of(y, hd)] = att_own[y, lanes_of(c, part), :]
    for r in range(1, t):
        ow_copy(r, landed=True).wait_recv()
        res_copy(r, landed=True).wait_recv()
    for i in range(len(att_list)):
        att_copy(i, landed=True).wait_recv()

    for cc in range(t):
        lanes = pl.ds(cc * cols, cols)
        mixed = jnp.zeros((part, cols), F32)
        for g in range(t):
            mixed = mixed + jnp.dot(
                att_all[g], ow[g, :, lanes], preferred_element_type=F32
            ).astype(BF16).astype(F32)
        pre[:, lanes] = ALPHA * res[cc].astype(F32) + mixed

    small = 64

    def norm_rows(i, _):
        at = aligned(i * small, small)
        v = pre[at, :]
        center = jnp.sum(v, axis=1, keepdims=True) / feat
        v = v - center
        spread = jnp.sum(v * v, axis=1, keepdims=True) / feat
        v = (v * lax.rsqrt(spread + EPSILON) * g1_ref[...] + b1_ref[...]).astype(BF16)
        first[m, c, 0, at, :] = v[:, :half_feat]
        first[m, c, 1, at, :] = v[:, half_feat:]
        return 0

    lax.fori_loop(0, part // small, norm_rows, 0)

    def member(r):
        return flip(m, r)

    def group_dev(r):
        return flip(s, r)

    def t1_copy(r, landed=False):
        ref = first.at[member(r) if landed else m, c, x]
        return remote(ref, ref, t1_send.at[r], t1_recv.at[r], sp=group_dev(r))

    def t2_copy(r, landed=False):
        ref = first.at[member(r), c, 1 - x if landed else x]
        return remote(ref, ref, t2_send.at[r], t2_recv.at[r], tp=across)

    def t3_copy(r, h, landed=False):
        xh = x if h == 0 else 1 - x
        ref = first.at[member(r), 1 - c if landed else c, xh]
        return remote(ref, ref, t3_send.at[r, h], t3_recv.at[r, h], tp=sibling)

    for r in range(GROUP - 1, 0, -1):
        t1_copy(r).start()
    for h in range(2):
        t3_copy(0, h).start()
    send_mat(1, False)
    send_mat(1, True)

    steps = (1, 2, 3)
    for r in range(1, n):
        w_copy(0, r, landed=True).wait_recv()

    def up_block(mm):
        def one(i, _):
            ch = i // 2
            lanes = aligned(lax.rem(i, 2) * (sub // 2), sub // 2)
            a = jnp.dot(
                first[mm, ch, 0], up[pl.ds(0, half_feat), lanes], preferred_element_type=F32
            ) + jnp.dot(
                first[mm, ch, 1],
                up[pl.ds(half_feat, half_feat), lanes],
                preferred_element_type=F32,
            )
            a = jnp.maximum(a, 0.0)
            act[aligned(mm * tok + ch * part, part), lanes] = (a * a).astype(BF16)
            return 0

        lax.fori_loop(0, 4, one, 0)

    for h in range(2):
        t3_copy(0, h, landed=True).wait_recv()
    for r in steps:
        t1_copy(r, landed=True).wait_recv()
        t2_copy(r).start()
        t3_copy(r, 0).start()
    up_block(m)
    for r in steps:
        t2_copy(r, landed=True).wait_recv()
        t3_copy(r, 1).start()
        for h in range(2):
            t3_copy(r, h, landed=True).wait_recv()
        up_block(member(r))

    def piece(mm, tq, fh):
        rows = aligned((tq * (cols // block) + fh) * block, block)
        return lax.dot_general(
            act[aligned(mm * tok, tok), :],
            down[rows, :],
            (((1,), (1,)), ((), ())),
            preferred_element_type=F32,
        )

    def pair_copy(p, mm):
        return remote(
            pair_out.at[p, mm],
            pair_in.at[p, mm],
            pair_send.at[p, mm],
            pair_recv.at[p, mm],
            tp=sibling,
        )

    def near_copy(p, r, landed=False):
        return remote(
            summed.at[p, member(r)],
            near_in.at[p, r],
            near_send.at[p, r],
            near_recv.at[p, r],
            sp=group_dev(r),
        )

    def cross_copy():
        return remote(cross_out, cross_in, cross_send.at[0], cross_recv.at[0], tp=across)

    member_order = (3, 1, 2, 0)

    def reduce_phase(p):
        xp = group if p == 0 else 1 - group
        far = range(half_n, n) if p else range(1, half_n)
        for r in far:
            w_copy(1, r, landed=True).wait_recv()
        for r in member_order:
            mm = member(r)
            for fh in range(cols // block):
                pair_out[p, mm, :, pl.ds(fh * block, block)] = piece(
                    mm, 2 * xp + 1 - c, fh
                ).astype(BF16)
            pair_copy(p, mm).start()
        for r in member_order:
            mm = member(r)
            pair_copy(p, mm).wait_recv()
            for fh in range(cols // block):
                lanes = pl.ds(fh * block, block)
                v = piece(mm, 2 * xp + c, fh) + pair_in[p, mm, :, lanes].astype(F32)
                summed[p, mm, :, lanes] = v.astype(BF16)
            if r:
                near_copy(p, r).start()

    def gather_phase(p):
        xp = group if p == 0 else 1 - group
        for r in range(1, GROUP):
            near_copy(p, r).wait_recv()

        def rows(i, _):
            at = aligned(i * 64, 64)
            v = summed[p, m, at, :].astype(F32)
            for r in range(1, GROUP):
                v = v + near_in[p, r, at, :].astype(F32)

            @pl.when(xp == x)
            def _():
                mixed_ref[at, :] = v

            @pl.when(xp != x)
            def _():
                cross_out[at, :] = v.astype(BF16)

            return 0

        lax.fori_loop(0, tok // 64, rows, 0)

        @pl.when(xp != x)
        def _():
            cross_copy().start()

    reduce_phase(0)
    reduce_phase(1)
    gather_phase(0)
    gather_phase(1)
    cross_copy().wait_recv()

    row_tile = 128
    for i in range(tok // row_tile):
        at = pl.ds(i * row_tile, row_tile)
        ch = i // (part // row_tile)
        inner = pl.ds((i % (part // row_tile)) * row_tile, row_tile)
        v = ALPHA * first[m, ch, x, inner, lanes_of(c, cols)].astype(F32)
        v = v + (mixed_ref[at, :] + cross_in[at, :].astype(F32))
        mixed_ref[at, :] = v
        sums = jnp.sum(v, axis=1, keepdims=True)
        squares = jnp.sum(v * v, axis=1, keepdims=True)
        lane = lax.broadcasted_iota(jnp.int32, (row_tile, 128), 1)
        st = jnp.where(lane == 0, sums, jnp.where(lane == 1, squares, 0.0))
        stat[q, :, at] = st.T[0:8, :]

    def stat_copy(r, landed=False):
        owner = flip(q, r) if landed else q
        return remote(
            stat.at[owner], stat.at[owner], stat_send.at[r], stat_recv.at[r], tp=flip(q, r)
        )

    for r in range(1, t):
        stat_copy(r).start()

    @pl.when(z < levels - 1)
    def _():
        def drain(slot, _):
            relay(slot).wait_send()
            return 0

        lax.fori_loop(0, 2 * z + 2, drain, 0)

    for cp in exchange():
        cp.wait_send()
    for r in range(1, n):
        br_copy(r).wait_send()
        w_copy(0, r).wait_send()
        w_copy(1, r).wait_send()
    for r in range(1, t):
        ow_copy(r).wait_send()
        res_copy(r).wait_send()
    for i in range(len(att_list)):
        att_copy(i).wait_send()
    for r in range(1, GROUP):
        t1_copy(r).wait_send()
        t2_copy(r).wait_send()
        for p in range(2):
            near_copy(p, r).wait_send()
    for r in range(GROUP):
        for h in range(2):
            t3_copy(r, h).wait_send()
        for p in range(2):
            pair_copy(p, r).wait_send()
    cross_copy().wait_send()

    for r in range(1, t):
        stat_copy(r, landed=True).wait_recv()
    for i in range(tok // row_tile):
        at = pl.ds(i * row_tile, row_tile)
        st = stat[0, :, at]
        for g in range(1, t):
            st = st + stat[g, :, at]
        st = jnp.concatenate([st, jnp.zeros((120, row_tile), F32)], axis=0).T
        center = st[:, 0:1] / feat
        spread = st[:, 1:2] / feat - center * center
        v = (mixed_ref[at, :] - center) * lax.rsqrt(spread + EPSILON)
        out_ref[at, :] = (v * g2_ref[q] + b2_ref[q]).astype(BF16)
    for r in range(1, t):
        stat_copy(r).wait_send()


def grouped_call(n, t, args):
    (
        queries,
        keys,
        values,
        breaks,
        residual_in,
        out_weight,
        first_gain,
        first_shift,
        up_weight,
        down_weight,
        second_gain,
        second_shift,
    ) = args
    tok, width = queries.shape
    heads = breaks.shape[1]
    hd = width // heads
    feat = out_weight.shape[1]
    cols = residual_in.shape[1]
    sub = up_weight.shape[1] // GROUP
    part = tok // 2
    br = jnp.pad(breaks.astype(F32).T, ((0, 8 - heads), (0, 0)))
    any_ = pl.BlockSpec(memory_space=pl.ANY)
    vmem = pl.BlockSpec(memory_space=pltpu.VMEM)
    dma = pltpu.SemaphoreType.DMA
    v = pltpu.VMEM
    return pl.pallas_call(
        functools.partial(grouped_kernel, n, t),
        out_shape=jax.ShapeDtypeStruct((tok, cols), BF16),
        in_specs=[any_] * 6 + [vmem, vmem, any_, any_, vmem, vmem],
        out_specs=vmem,
        scratch_shapes=[
            v((n, tok, 2 * hd), BF16),
            v((2, tok, hd), BF16),
            v((n, 8, tok), F32),
            v((2, tok, 128), F32),
            v((2, tok, hd), F32),
            v((2, tok, hd), BF16),
            v((t, part, width), BF16),
            v((256, 256), BF16),
            v((t, width, feat), BF16),
            v((t, part, cols), BF16),
            v((part, feat), F32),
            v((GROUP, 2, 2, part, feat // 2), BF16),
            v((feat, sub), BF16),
            v((feat, sub), BF16),
            v((GROUP * tok, sub), BF16),
            v((2, GROUP, tok, cols), BF16),
            v((2, GROUP, tok, cols), BF16),
            v((2, GROUP, tok, cols), BF16),
            v((2, GROUP, tok, cols), BF16),
            v((tok, cols), BF16),
            v((tok, cols), BF16),
            v((tok, cols), F32),
            v((t, 8, tok), F32),
            dma((n,)),
            dma((n,)),
            dma((3,)),
            dma((3,)),
            dma((n,)),
            dma((n,)),
            dma((t,)),
            dma((t,)),
            dma((t,)),
            dma((t,)),
            dma((2 * t - 1,)),
            dma((2 * t - 1,)),
            dma((2, n)),
            dma((2, n)),
            dma((GROUP,)),
            dma((GROUP,)),
            dma((GROUP,)),
            dma((GROUP,)),
            dma((GROUP, 2)),
            dma((GROUP, 2)),
            dma((2, GROUP)),
            dma((2, GROUP)),
            dma((2, GROUP)),
            dma((2, GROUP)),
            dma((1,)),
            dma((1,)),
            dma((t,)),
            dma((t,)),
            dma((8,)),
            pltpu.SemaphoreType.REGULAR,
        ],
        compiler_params=pltpu.CompilerParams(
            collective_id=0, has_side_effects=True, vmem_limit_bytes=62 * 1024 * 1024
        ),
    )(
        queries,
        keys,
        values,
        br,
        residual_in,
        out_weight,
        first_gain.reshape(1, feat),
        first_shift.reshape(1, feat),
        up_weight,
        down_weight,
        second_gain.reshape(t, 1, cols),
        second_shift.reshape(t, 1, cols),
    )


def solution(mesh):
    n, t = mesh.shape["sp"], mesh.shape["tp"]

    def body(
        queries,
        keys,
        values,
        breaks,
        residual_in,
        out_weight,
        first_gain,
        first_shift,
        up_weight,
        down_weight,
        second_gain,
        second_shift,
    ):
        tok, width = queries.shape
        heads = breaks.shape[1]
        if heads == 2 and t == 4 and n == 2 * GROUP:
            return grouped_call(
                n,
                t,
                (
                    queries,
                    keys,
                    values,
                    breaks,
                    residual_in,
                    out_weight,
                    first_gain,
                    first_shift,
                    up_weight,
                    down_weight,
                    second_gain,
                    second_shift,
                ),
            )
        feat = out_weight.shape[1]
        cols = residual_in.shape[1]
        hidden = up_weight.shape[1]
        block = up_weight.shape[0]
        per = n // t
        kv = jnp.concatenate([keys, values], axis=1)
        br = jnp.pad(breaks.astype(F32).T, ((0, 8 - heads), (0, 0)))
        any_ = pl.BlockSpec(memory_space=pl.ANY)
        vmem = pl.BlockSpec(memory_space=pltpu.VMEM)
        dma = pltpu.SemaphoreType.DMA
        ring = dma((3, 2, n // 2 + 1, 2))
        return pl.pallas_call(
            functools.partial(layer_kernel, n, t, heads),
            out_shape=jax.ShapeDtypeStruct((tok, cols), BF16),
            in_specs=[vmem, any_, any_, any_, any_, vmem, vmem, any_, any_, vmem, vmem],
            out_specs=vmem,
            scratch_shapes=[
                pltpu.VMEM((n * tok, 2 * width), BF16),
                pltpu.VMEM((feat, hidden), BF16),
                pltpu.VMEM((feat, hidden), BF16),
                pltpu.VMEM((n, 8, tok), F32),
                pltpu.VMEM((t, width, feat), BF16),
                pltpu.VMEM((t, tok, cols), BF16),
                pltpu.VMEM((heads, tok, 128), F32),
                pltpu.VMEM((tok, width), F32),
                pltpu.VMEM((t, tok, width), BF16),
                pltpu.VMEM((tok, tok), BF16),
                pltpu.VMEM((tok, feat), F32),
                pltpu.VMEM((tok, feat), BF16),
                pltpu.VMEM((tok, hidden), BF16),
                pltpu.VMEM((n, tok, block), BF16),
                pltpu.VMEM((t, per, tok, block), BF16),
                pltpu.VMEM((t, 8, tok), F32),
                ring,
                ring,
                dma((n,)),
                dma((n,)),
                dma((t,)),
                dma((t,)),
                dma((t,)),
                dma((t,)),
                dma((t,)),
                dma((t,)),
                dma((n,)),
                dma((t, per)),
                dma((t,)),
                dma((t,)),
                dma((6,)),
            ],
            compiler_params=pltpu.CompilerParams(
                collective_id=0, has_side_effects=True, vmem_limit_bytes=62 * 1024 * 1024
            ),
        )(
            queries,
            kv,
            br,
            residual_in,
            out_weight,
            first_gain.reshape(1, feat),
            first_shift.reshape(1, feat),
            up_weight,
            down_weight,
            second_gain.reshape(t, 1, cols),
            second_shift.reshape(t, 1, cols),
        )

    return jax.shard_map(
        body,
        mesh=mesh,
        in_specs=(
            P("sp", "tp"),
            P("sp", "tp"),
            P("sp", "tp"),
            P("sp", "tp"),
            P("sp", "tp"),
            P("tp", None),
            P(),
            P(),
            P("sp", "tp"),
            P("sp", "tp"),
            P(),
            P(),
        ),
        out_specs=P("sp", "tp"),
        check_vma=False,
    )
```

```python
import functools

import jax
import jax.numpy as jnp
from jax import lax
from jax.experimental import pallas as pl
from jax.experimental.pallas import tpu as pltpu
from jax.sharding import PartitionSpec as P

ALPHA = 2.0**0.25
EPSILON = 1e-05
MESH = pl.DeviceIdType.MESH
F32 = jnp.float32
BF16 = jnp.bfloat16
KV, UP, DOWN = 0, 1, 2
RIGHT, LEFT = 0, 1


def aligned(start, size):
    return pl.ds(pl.multiple_of(start, size), size)


def layer_kernel(
    n,
    t,
    heads,
    q_ref,
    kv_in,
    br_in,
    res_in,
    ow_in,
    g1_ref,
    b1_ref,
    up_in,
    down_in,
    g2_ref,
    b2_ref,
    out_ref,
    kv,
    up,
    down,
    br,
    ow,
    res,
    later_sum,
    totals,
    att_all,
    lower,
    pre,
    first,
    activated,
    part,
    mix,
    stat,
    ring_send,
    ring_recv,
    br_send,
    br_recv,
    ow_send,
    ow_recv,
    res_send,
    res_recv,
    att_send,
    att_recv,
    mix_send,
    mix_recv,
    stat_send,
    stat_recv,
    local_sem,
):
    me = lax.axis_index("sp")
    me_t = lax.axis_index("tp")
    tok = q_ref.shape[0]
    width = q_ref.shape[1]
    hd = width // heads
    feat = first.shape[1]
    cols = feat // t
    block = feat // n
    per = n // t
    half_n = n // 2

    def at_pos(p):
        p = lax.rem(p + n, n)
        back = p // half_n
        return 2 * (p + back * (n - 1 - 2 * p)) + back

    pos = me // 2 + lax.rem(me, 2) * (n - 1 - 2 * (me // 2))
    next_dev = (at_pos(pos + 1), at_pos(pos - 1))
    own_in = (kv_in, up_in, down_in)
    full = (kv, up, down)
    rows_of = (tok, block, block)

    def ring_copy(item, way, hop, piece, own=False):
        rows = rows_of[item]
        half = rows // 2
        owner = at_pos(pos - (hop - 1) if way == RIGHT else pos + (hop - 1))
        dst = full[item].at[aligned(owner * rows + piece * half, half)]
        src = own_in[item].at[aligned(piece * half, half)] if own else dst
        return pltpu.make_async_remote_copy(
            src_ref=src,
            dst_ref=dst,
            send_sem=ring_send.at[item, way, hop, piece],
            recv_sem=ring_recv.at[item, way, hop, piece],
            device_id={"sp": next_dev[way]},
            device_id_type=MESH,
        )

    def ring_landed(item, way, hop, piece):
        rows = rows_of[item]
        half = rows // 2
        owner = at_pos(pos - hop if way == RIGHT else pos + hop)
        dst = full[item].at[aligned(owner * rows + piece * half, half)]
        return pltpu.make_async_remote_copy(
            src_ref=dst,
            dst_ref=dst,
            send_sem=ring_send.at[item, way, hop, piece],
            recv_sem=ring_recv.at[item, way, hop, piece],
            device_id={"sp": next_dev[way]},
            device_id_type=MESH,
        )

    def start_own(item):
        ring_copy(item, RIGHT, 1, 0, own=True).start()
        ring_copy(item, LEFT, 1, 1, own=True).start()
        ring_copy(item, RIGHT, 1, 1, own=True).start()
        ring_copy(item, LEFT, 1, 0, own=True).start()

    def event(item, e, hop=None, second=None):
        static = isinstance(e, int)
        hop = 1 + e // 2
        second = e % 2 if static else lax.rem(e, 2)
        ring_landed(item, RIGHT, hop, second).wait_recv()

        def forward_right():
            ring_copy(item, RIGHT, hop + 1, second).start()

        def forward_left():
            ring_copy(item, LEFT, hop + 1, 1 - second).start()

        def start_next():
            if item < DOWN:
                start_own(item + 1)

        def guarded(cond, fn):
            if static:
                if cond:
                    fn()
            else:
                pl.when(cond)(fn)

        guarded(e < n - 3, forward_right)
        ring_landed(item, LEFT, hop, 1 - second).wait_recv()
        guarded(e < n - 3, forward_left)
        guarded(e == n - 4, start_next)

    def drain_sends(item):
        def one(e, _):
            hop = 1 + e // 2
            second = lax.rem(e, 2)
            ring_copy(item, RIGHT, hop, second).wait_send()
            ring_copy(item, LEFT, hop, 1 - second).wait_send()
            return 0

        lax.fori_loop(0, n - 1, one, 0)

    def peer_t(d):
        return lax.rem(me_t + d, t)

    def tp_copy(src, dst_of, sends, recvs, d):
        return pltpu.make_async_remote_copy(
            src_ref=src,
            dst_ref=dst_of(me_t),
            send_sem=sends.at[d],
            recv_sem=recvs.at[d],
            device_id={"tp": peer_t(d)},
            device_id_type=MESH,
        )

    def tp_landed(dst_of, sends, recvs, d):
        dst = dst_of(lax.rem(me_t + t - d, t))
        return pltpu.make_async_remote_copy(
            src_ref=dst,
            dst_ref=dst,
            send_sem=sends.at[d],
            recv_sem=recvs.at[d],
            device_id={"tp": peer_t(d)},
            device_id_type=MESH,
        )

    def br_copy(d, landed=False):
        owner = lax.rem(me + n - d, n) if landed else me
        return pltpu.make_async_remote_copy(
            src_ref=br.at[owner] if landed else br_in,
            dst_ref=br.at[owner],
            send_sem=br_send.at[d],
            recv_sem=br_recv.at[d],
            device_id={"sp": lax.rem(me + d, n)},
            device_id_type=MESH,
        )

    barrier = pltpu.get_barrier_semaphore()

    def greet(d, _):
        pl.semaphore_signal(
            barrier, inc=1, device_id={"sp": lax.rem(me + d, n)}, device_id_type=MESH
        )
        return 0

    lax.fori_loop(1, n, greet, 0)
    for d in range(1, t):
        pl.semaphore_signal(barrier, inc=1, device_id={"tp": peer_t(d)}, device_id_type=MESH)

    res_at = lambda g: res.at[g]
    ow_at = lambda g: ow.at[g]
    att_at = lambda g: att_all.at[g]

    locals_ = [
        pltpu.make_async_copy(kv_in, kv.at[aligned(me * tok, tok)], local_sem.at[0]),
        pltpu.make_async_copy(up_in, up.at[aligned(me * block, block)], local_sem.at[1]),
        pltpu.make_async_copy(down_in, down.at[aligned(me * block, block)], local_sem.at[2]),
        pltpu.make_async_copy(br_in, br.at[me], local_sem.at[3]),
        pltpu.make_async_copy(res_in, res.at[me_t], local_sem.at[4]),
        pltpu.make_async_copy(ow_in, ow.at[me_t], local_sem.at[5]),
    ]
    pl.semaphore_wait(barrier, n - 1 + t - 1)
    start_own(KV)

    def send_breaks(d, _):
        br_copy(d).start()
        return 0

    lax.fori_loop(1, n, send_breaks, 0)
    for c in locals_:
        c.start()
    for d in range(1, t):
        tp_copy(ow_in, ow_at, ow_send, ow_recv, d).start()
    for d in range(1, t):
        tp_copy(res_in, res_at, res_send, res_recv, d).start()

    key_row = lax.broadcasted_iota(jnp.int32, (tok, tok), 0)
    key_col = lax.broadcasted_iota(jnp.int32, (tok, tok), 1)
    lower[...] = jnp.where(key_row > key_col, 1.0, 0.0).astype(BF16)
    later_sum[...] = jnp.zeros_like(later_sum)
    totals[...] = jnp.zeros_like(totals)

    def kv_event(e, _):
        event(KV, e)
        return 0

    lax.fori_loop(0, n - 2, kv_event, 0)

    def last_event(item):
        ring_landed(item, RIGHT, half_n, 0).wait_recv()
        ring_landed(item, LEFT, half_n, 1).wait_recv()

    last_event(KV)

    def wait_breaks(d, _):
        br_copy(d, landed=True).wait_recv()
        return 0

    lax.fori_loop(1, n, wait_breaks, 0)
    for c in locals_:
        c.wait()

    scale = hd ** (-0.5)
    tile = 128

    def attend_block(j):
        b = me - j
        for h in range(heads):
            def rows(i, _):
                at = aligned(i * tile, tile)
                keys = kv[aligned(b * tok, tok), pl.ds(h * hd, hd)]
                vals = kv[aligned(b * tok, tok), pl.ds(width + h * hd, hd)]
                z = lax.dot_general(
                    q_ref[at, pl.ds(h * hd, hd)],
                    keys,
                    (((1,), (1,)), ((), ())),
                    preferred_element_type=F32,
                )
                z = z * scale + br[b, pl.ds(h, 1), :]
                soft = jnp.log(1.0 + jnp.exp(-jnp.abs(z)))
                log_break = jnp.minimum(z, 0.0) - soft
                r = lax.broadcasted_iota(jnp.int32, (tile, tok), 0) + i * tile + j * tok
                strict = lax.broadcasted_iota(jnp.int32, (tile, tok), 1) < r
                log_keep = jnp.where(strict, log_break - z, 0.0)
                high = log_keep.astype(BF16)
                low = (log_keep - high.astype(F32)).astype(BF16)
                tri = lower[...]
                later = jnp.dot(high, tri, preferred_element_type=F32) + jnp.dot(
                    low, tri, preferred_element_type=F32
                )
                before = later_sum[h, at, :]
                w = jnp.exp(log_break + later + before[:, 0:1])
                w = jnp.where(strict, w, 0.0).astype(BF16)
                totals[at, pl.ds(h * hd, hd)] += jnp.dot(w, vals, preferred_element_type=F32)
                later_sum[h, at, :] = before + jnp.sum(log_keep, axis=1, keepdims=True)
                return 0

            lax.fori_loop(0, tok // tile, rows, 0)

    def attend_step(j, _):
        @pl.when(j <= me)
        def _():
            attend_block(j)

        @pl.when(j < n - 2)
        def _():
            event(UP, j)

        return 0

    lax.fori_loop(0, n, attend_step, 0)

    own_att = att_all.at[me_t]
    own_att[...] = totals[...].astype(BF16)
    for d in range(1, t):
        tp_copy(own_att, att_at, att_send, att_recv, d).start()
    last_event(UP)
    for d in range(1, t):
        tp_landed(ow_at, ow_send, ow_recv, d).wait_recv()
        tp_landed(res_at, res_send, res_recv, d).wait_recv()
    for d in range(1, t):
        tp_landed(att_at, att_send, att_recv, d).wait_recv()

    big = 256

    def mix_rows(i, _):
        at = aligned(i * big, big)
        for c in range(t):
            lanes = pl.ds(c * cols, cols)
            acc = ALPHA * res[c, at, :].astype(F32)
            mixed = jnp.zeros((big, cols), F32)
            for g in range(t):
                mixed = mixed + jnp.dot(
                    att_all[g, at, :], ow[g, :, lanes], preferred_element_type=F32
                ).astype(BF16).astype(F32)
            pre[at, lanes] = acc + mixed
        return 0

    lax.fori_loop(0, tok // big, mix_rows, 0)
    event(DOWN, 0)

    small = 64

    def norm_rows(i, _):
        at = aligned(i * small, small)
        x = pre[at, :]
        center = jnp.sum(x, axis=1, keepdims=True) / feat
        x = x - center
        spread = jnp.sum(x * x, axis=1, keepdims=True) / feat
        first[at, :] = (x * lax.rsqrt(spread + EPSILON) * g1_ref[...] + b1_ref[...]).astype(BF16)
        return 0

    lax.fori_loop(0, tok // small, norm_rows, 0)

    hidden = up.shape[1]
    strip = 256

    def up_cols(i, _):
        lanes = aligned(i * strip, strip)
        a = jnp.dot(first[...], up[:, lanes], preferred_element_type=F32)
        a = jnp.maximum(a, 0.0)
        activated[:, lanes] = (a * a).astype(BF16)
        return 0

    event(DOWN, 1)
    lax.fori_loop(0, hidden // strip, up_cols, 0)

    def mix_copy(s):
        k = lax.rem(s, per)
        owner = s // per
        return owner, pltpu.make_async_remote_copy(
            src_ref=part.at[s],
            dst_ref=mix.at[me_t, k],
            send_sem=mix_send.at[s],
            recv_sem=mix_recv.at[me_t, k],
            device_id={"tp": owner},
            device_id_type=MESH,
        )

    def down_block(s):
        y = lax.dot_general(
            activated[...],
            down[aligned(s * block, block), :],
            (((1,), (1,)), ((), ())),
            preferred_element_type=F32,
        ).astype(BF16)
        owner, copy = mix_copy(s)

        @pl.when(owner == me_t)
        def _():
            mix[me_t, lax.rem(s, per)] = y

        @pl.when(owner != me_t)
        def _():
            part[s] = y
            copy.start()

    down_block(me)

    def down_step(h, _):
        @pl.when(h > 1)
        def _():
            event(DOWN, 2 * h - 2)
            event(DOWN, 2 * h - 1)

        def side(w, _):
            down_block(at_pos(pos + (2 * w - 1) * h))
            return 0

        lax.fori_loop(0, 2, side, 0)
        return 0

    lax.fori_loop(1, half_n, down_step, 0)
    last_event(DOWN)
    down_block(at_pos(pos + half_n))

    def mix_wait(s, _):
        owner, copy = mix_copy(s)

        @pl.when(owner != me_t)
        def _():
            copy.wait_send()

        return 0

    for d in range(1, t):
        g = lax.rem(me_t + t - d, t)
        for k in range(per):
            dst = mix.at[g, k]
            pltpu.make_async_remote_copy(
                src_ref=dst,
                dst_ref=dst,
                send_sem=mix_send.at[0],
                recv_sem=mix_recv.at[g, k],
                device_id={"tp": peer_t(d)},
                device_id_type=MESH,
            ).wait_recv()

    def second_pre(i, _):
        at = aligned(i * 128, 128)
        sums = jnp.zeros((128, 1), F32)
        squares = jnp.zeros((128, 1), F32)
        x = ALPHA * first[at, aligned(me_t * cols, cols)].astype(F32)
        pieces = []
        for k in range(per):
            v = mix[0, k, at, :].astype(F32)
            for g in range(1, t):
                v = v + mix[g, k, at, :].astype(F32)
            pieces.append(v)
        x = x + (jnp.concatenate(pieces, axis=1) if per > 1 else pieces[0])
        pre[at, pl.ds(0, cols)] = x
        sums = jnp.sum(x, axis=1, keepdims=True)
        squares = jnp.sum(x * x, axis=1, keepdims=True)
        lane = lax.broadcasted_iota(jnp.int32, (128, 128), 1)
        s = jnp.where(lane == 0, sums, jnp.where(lane == 1, squares, 0.0))
        stat[me_t, :, at] = s.T[0:8, :]
        return 0

    for i in range(tok // 128):
        second_pre(i, 0)
    stat_at = lambda g: stat.at[g]
    for d in range(1, t):
        tp_copy(stat.at[me_t], stat_at, stat_send, stat_recv, d).start()

    lax.fori_loop(0, n, mix_wait, 0)
    for item in (KV, UP, DOWN):
        drain_sends(item)

    def br_done(d, _):
        br_copy(d).wait_send()
        return 0

    lax.fori_loop(1, n, br_done, 0)
    for d in range(1, t):
        tp_copy(ow_in, ow_at, ow_send, ow_recv, d).wait_send()
        tp_copy(res_in, res_at, res_send, res_recv, d).wait_send()
        tp_copy(own_att, att_at, att_send, att_recv, d).wait_send()
    for d in range(1, t):
        tp_landed(stat_at, stat_send, stat_recv, d).wait_recv()

    for i in range(tok // 128):
        at = pl.ds(i * 128, 128)
        s = stat[0, :, at]
        for g in range(1, t):
            s = s + stat[g, :, at]
        s = jnp.concatenate([s, jnp.zeros((120, 128), F32)], axis=0).T
        center = s[:, 0:1] / feat
        spread = s[:, 1:2] / feat - center * center
        x = pre[at, pl.ds(0, cols)]
        x = (x - center) * lax.rsqrt(spread + EPSILON)
        out_ref[at, :] = (x * g2_ref[me_t] + b2_ref[me_t]).astype(BF16)
    for d in range(1, t):
        tp_copy(stat.at[me_t], stat_at, stat_send, stat_recv, d).wait_send()


GROUP = 4


def flip(a, r):
    bit = 1
    out = a
    while bit <= r:
        if r & bit:
            out = out + bit - 2 * bit * lax.rem(a // bit, 2)
        bit *= 2
    return out


def remote(src, dst, send, recv, **where):
    return pltpu.make_async_remote_copy(
        src_ref=src,
        dst_ref=dst,
        send_sem=send,
        recv_sem=recv,
        device_id=where,
        device_id_type=MESH,
    )


def grouped_kernel(
    n,
    t,
    q_in,
    k_in,
    v_in,
    br_in,
    res_in,
    ow_in,
    g1_ref,
    b1_ref,
    up_in,
    down_in,
    g2_ref,
    b2_ref,
    out_ref,
    kvb,
    qb,
    br,
    later_sum,
    totals,
    att_own,
    att_all,
    tri_ref,
    ow,
    res,
    pre,
    first,
    up,
    down,
    act,
    pair_out,
    pair_in,
    summed,
    near_in,
    held,
    side_out,
    side_in,
    cross_out,
    cross_in,
    mixed_ref,
    stat,
    kv_send,
    kv_recv,
    kx_send,
    kx_recv,
    br_send,
    br_recv,
    ow_send,
    ow_recv,
    res_send,
    res_recv,
    att_send,
    att_recv,
    w_send,
    w_recv,
    t1_send,
    t1_recv,
    t2_send,
    t2_recv,
    t3_send,
    t3_recv,
    pair_send,
    pair_recv,
    near_send,
    near_recv,
    side_send,
    side_recv,
    cross_send,
    cross_recv,
    stat_send,
    stat_recv,
    local_sem,
    go_sem,
):
    s = lax.axis_index("sp")
    q = lax.axis_index("tp")
    y = lax.rem(s, 2)
    z = s // 2
    levels = n // 2
    m = lax.rem(s, GROUP)
    group = s // GROUP
    x = q // 2
    c = lax.rem(q, 2)
    tok, width = q_in.shape
    hd = width // 2
    feat = ow.shape[2]
    cols = feat // t
    half_feat = feat // 2
    block = up_in.shape[0]
    sub = up_in.shape[1] // GROUP
    part = tok // 2
    half_n = n // 2
    sibling = flip(q, 1)
    across = flip(q, 2)

    barrier = pltpu.get_barrier_semaphore()
    for r in range(1, n):
        pl.semaphore_signal(barrier, inc=1, device_id={"sp": flip(s, r)}, device_id_type=MESH)
    for r in range(1, t):
        pl.semaphore_signal(barrier, inc=1, device_id={"tp": flip(q, r)}, device_id_type=MESH)
        pl.semaphore_signal(
            barrier, inc=1, device_id={"sp": flip(s, 1), "tp": flip(q, r)}, device_id_type=MESH
        )

    def lanes_of(i, size):
        return aligned(i * size, size)

    own_copies = [
        pltpu.make_async_copy(
            k_in.at[:, lanes_of(y, hd)], kvb.at[s, :, pl.ds(0, hd)], local_sem.at[0]
        ),
        pltpu.make_async_copy(
            v_in.at[:, lanes_of(y, hd)], kvb.at[s, :, pl.ds(hd, hd)], local_sem.at[1]
        ),
        pltpu.make_async_copy(q_in.at[:, lanes_of(y, hd)], qb.at[y], local_sem.at[2]),
    ]
    other_copies = [
        pltpu.make_async_copy(br_in, br.at[s], local_sem.at[3]),
        pltpu.make_async_copy(res_in.at[lanes_of(c, part)], res.at[q], local_sem.at[4]),
        pltpu.make_async_copy(ow_in, ow.at[q], local_sem.at[5]),
        pltpu.make_async_copy(
            up_in.at[:, lanes_of(m, sub)], up.at[lanes_of(s, block)], local_sem.at[6]
        ),
        pltpu.make_async_copy(
            down_in.at[:, lanes_of(m, sub)], down.at[lanes_of(s, block)], local_sem.at[7]
        ),
    ]
    for cp in own_copies:
        cp.start()

    ps = flip(s, 1)
    py = 1 - y

    def exchange(landed=False):
        own = ps if landed else s
        row = y if landed else py
        mine = py if landed else y
        return [
            remote(
                kvb.at[own, :, pl.ds(0, hd)] if landed else k_in.at[:, lanes_of(row, hd)],
                kvb.at[own, :, pl.ds(0, hd)],
                kx_send.at[0],
                kx_recv.at[0],
                sp=ps,
            ),
            remote(
                kvb.at[own, :, pl.ds(hd, hd)] if landed else v_in.at[:, lanes_of(row, hd)],
                kvb.at[own, :, pl.ds(hd, hd)],
                kx_send.at[1],
                kx_recv.at[1],
                sp=ps,
            ),
            remote(
                qb.at[mine] if landed else q_in.at[:, lanes_of(row, hd)],
                qb.at[mine],
                kx_send.at[2],
                kx_recv.at[2],
                sp=ps,
            ),
        ]

    def relay(slot):
        return remote(kvb.at[slot], kvb.at[slot], kv_send.at[slot], kv_recv.at[slot], sp=s + 2)

    def relay_landed(slot):
        return remote(kvb.at[slot], kvb.at[slot], kv_send.at[slot], kv_recv.at[slot], sp=s)

    def br_copy(r, landed=False):
        owner = flip(s, r) if landed else s
        return remote(
            br.at[owner] if landed else br_in,
            br.at[owner],
            br_send.at[r],
            br_recv.at[owner],
            sp=flip(s, r),
        )

    def ow_copy(r, landed=False):
        owner = flip(q, r) if landed else q
        return remote(
            ow.at[owner] if landed else ow_in,
            ow.at[owner],
            ow_send.at[r],
            ow_recv.at[r],
            tp=flip(q, r),
        )

    def ow_pass(landed=False):
        ref = ow.at[flip(q, 3) if landed else across]
        return remote(ref, ref, ow_send.at[3], ow_recv.at[3], tp=sibling)

    def res_copy(r, landed=False):
        to = flip(q, r)
        owner = to if landed else q
        return remote(
            res.at[owner] if landed else res_in.at[lanes_of(lax.rem(to, 2), part)],
            res.at[owner],
            res_send.at[r],
            res_recv.at[r],
            tp=to,
        )

    mats_in = (up_in, down_in)
    mats = (up, down)

    def w_copy(mat, r, landed=False):
        to = flip(s, r)
        owner = to if landed else s
        dst = mats[mat].at[lanes_of(owner, block)]
        return remote(
            dst if landed else mats_in[mat].at[:, lanes_of(lax.rem(to, GROUP), sub)],
            dst,
            w_send.at[mat, r],
            w_recv.at[mat, r],
            sp=to,
        )

    def climbs(r):
        return lax.rem(s // (half_n if r >= half_n else 2), 2) == 0

    def send_mat(mat, rs, upward):
        for r in rs:

            def go(r=r):
                w_copy(mat, r).start()

            if r < 2:
                go()
            else:
                pl.when(climbs(r) if upward else jnp.logical_not(climbs(r)))(go)

    def send_up(mat, skip=()):
        far_level = [r for r in range(half_n, n) if (r // 2) % 2 and r not in skip]
        same_level = [r for r in range(half_n, n) if not (r // 2) % 2 and r not in skip]

        @pl.when(group == 0)
        def _():
            @pl.when(lax.rem(z, 2) == 0)
            def _():
                for r in same_level + far_level:
                    w_copy(mat, r).start()

            @pl.when(lax.rem(z, 2) == 1)
            def _():
                for r in far_level + same_level:
                    w_copy(mat, r).start()

        send_mat(mat, (2, 3), True)

    straight = [r for r in range(n - 1, 0, -1) if r % 2 == 0]
    turning = [r for r in range(n - 1, 0, -1) if r % 2]

    pl.semaphore_wait(barrier, n - 1 + 2 * (t - 1))
    for cp in exchange():
        cp.start()
    for r in range(1, n):
        br_copy(r).start()
    for cp in other_copies:
        cp.start()
    for cp in own_copies:
        cp.wait()

    @pl.when(z < levels - 1)
    def _():
        relay(s).start()

    for r in range(1, t):
        res_copy(r).start()
    for r in (1, 2):
        ow_copy(r).start()
    send_mat(0, straight, False)

    inner = lax.rem(z, 2) != group
    far_straight = [r for r in straight if r >= half_n]

    @pl.when(inner)
    def _():
        send_mat(1, far_straight, False)

    key_row = lax.broadcasted_iota(jnp.int32, tri_ref.shape, 0)
    key_col = lax.broadcasted_iota(jnp.int32, tri_ref.shape, 1)
    tri_ref[...] = jnp.where(key_row > key_col, 1.0, 0.0).astype(BF16)
    later_sum[...] = jnp.zeros_like(later_sum)
    totals[...] = jnp.zeros_like(totals)

    for cp in other_copies:
        cp.wait()

    def br_landed(slot):
        remote(br.at[slot], br.at[slot], br_send.at[0], br_recv.at[slot], sp=s).wait_recv()

    scale = hd ** (-0.5)
    tile = 128
    span = tri_ref.shape[0]

    def attend(slot, qy, masked):
        def rows(i, _):
            at = aligned(i * tile, tile)
            z_ = lax.dot_general(
                qb[qy, at, :],
                kvb[slot, :, pl.ds(0, hd)],
                (((1,), (1,)), ((), ())),
                preferred_element_type=F32,
            )
            z_ = z_ * scale + br[slot, pl.ds(y, 1), :]
            soft = jnp.log(1.0 + jnp.exp(-jnp.abs(z_)))
            log_break = jnp.minimum(z_, 0.0) - soft
            keep = log_break - z_
            if masked:
                r = lax.broadcasted_iota(jnp.int32, (tile, tok), 0) + i * tile
                strict = lax.broadcasted_iota(jnp.int32, (tile, tok), 1) < r
                keep = jnp.where(strict, keep, 0.0)
            high = keep.astype(BF16)
            low = (keep - high.astype(F32)).astype(BF16)
            tri = tri_ref[...]
            run = later_sum[qy, at, :][:, 0:1]
            pieces = []
            for b in range(tok // span - 1, -1, -1):
                sl = slice(b * span, (b + 1) * span)
                later = jnp.dot(high[:, sl], tri, preferred_element_type=F32) + jnp.dot(
                    low[:, sl], tri, preferred_element_type=F32
                )
                pieces.append(later + run)
                run = run + jnp.sum(keep[:, sl], axis=1, keepdims=True)
            w = jnp.exp(log_break + jnp.concatenate(pieces[::-1], axis=1))
            if masked:
                w = jnp.where(strict, w, 0.0)
            totals[qy, at, :] += jnp.dot(
                w.astype(BF16), kvb[slot, :, pl.ds(hd, hd)], preferred_element_type=F32
            )
            later_sum[qy, at, :] = jnp.broadcast_to(run, (tile, 128))
            return 0

        lax.fori_loop(0, tok // tile, rows, 0)

    attend(s, y, True)
    for cp in exchange(landed=True):
        cp.wait_recv()

    @pl.when(z < levels - 1)
    def _():
        relay(ps).start()

    br_landed(ps)
    send_mat(0, turning, False)
    attend(ps, py, True)

    def fetch(slot):
        @pl.when(slot >= 0)
        def _():
            relay_landed(slot).wait_recv()
            br_landed(slot)

            @pl.when(z < levels - 1)
            def _():
                relay(slot).start()

    ahead = jnp.where(z < levels - 1, 2, 0)

    @pl.when(z < levels - 1)
    def _():
        fetch(2 * z - 1)

    attend(2 * z, 1, False)

    @pl.when(z < levels - 1)
    def _():
        fetch(2 * z - 2)

    def attend_step(k, _):
        slot = 2 * z + 1 - k
        fetch(slot - ahead)

        @pl.when(slot >= 0)
        def _():
            def one(qy, _):
                attend(slot, qy, False)
                return 0

            lax.fori_loop(0, 2, one, 0)

        return 0

    lax.fori_loop(2, n, attend_step, 0)

    @pl.when(z < levels - 1)
    def _():
        def drain(slot, _):
            relay(slot).wait_send()
            return 0

        lax.fori_loop(0, 2 * z + 2, drain, 0)

    @pl.when(z == 1)
    def _():
        pl.semaphore_signal(go_sem, inc=1, device_id={"sp": s - 2}, device_id_type=MESH)

    @pl.when(z == 0)
    def _():
        pl.semaphore_wait(go_sem, 1)

    send_up(0)

    @pl.when(inner)
    def _():
        send_mat(1, far_straight, True)

    ow_copy(2, landed=True).wait_recv()
    ow_pass().start()

    att_own[...] = totals[...].astype(BF16)
    att_list = [(dy, r) for dy in range(2) for r in range(t) if dy or r]

    def att_copy(i, landed=False):
        dy, r = att_list[i]
        ty = flip(y, 1) if dy else y
        tq = flip(q, r)
        sp = ps if dy else s
        if landed:
            dst = att_all.at[tq, :, lanes_of(ty, hd)]
            return remote(dst, dst, att_send.at[i], att_recv.at[i], sp=sp, tp=tq)
        return remote(
            att_own.at[ty, lanes_of(lax.rem(tq, 2), part)],
            att_all.at[q, :, lanes_of(y, hd)],
            att_send.at[i],
            att_recv.at[i],
            sp=sp,
            tp=tq,
        )

    for i in range(len(att_list)):
        att_copy(i).start()
    att_all[q, :, lanes_of(y, hd)] = att_own[y, lanes_of(c, part), :]
    ow_copy(1, landed=True).wait_recv()
    ow_pass(landed=True).wait_recv()
    for r in range(1, t):
        res_copy(r, landed=True).wait_recv()
    for i in range(len(att_list)):
        att_copy(i, landed=True).wait_recv()

    for cc in range(t):
        lanes = pl.ds(cc * cols, cols)
        mixed = jnp.zeros((part, cols), F32)
        for g in range(t):
            mixed = mixed + jnp.dot(
                att_all[g], ow[g, :, lanes], preferred_element_type=F32
            ).astype(BF16).astype(F32)
        pre[:, lanes] = ALPHA * res[cc].astype(F32) + mixed

    small = 64

    def norm_rows(i, _):
        at = aligned(i * small, small)
        v = pre[at, :]
        center = jnp.sum(v, axis=1, keepdims=True) / feat
        v = v - center
        spread = jnp.sum(v * v, axis=1, keepdims=True) / feat
        v = (v * lax.rsqrt(spread + EPSILON) * g1_ref[...] + b1_ref[...]).astype(BF16)
        first[m, c, 0, at, :] = v[:, :half_feat]
        first[m, c, 1, at, :] = v[:, half_feat:]
        return 0

    lax.fori_loop(0, part // small, norm_rows, 0)

    def member(r):
        return flip(m, r)

    def group_dev(r):
        return flip(s, r)

    quarter = part // 2

    def t1_copy(r, e, landed=False):
        owner = member(r) if landed else (member(2) if r == 3 else m)
        ref = first.at[owner, c, x, pl.ds(e * quarter, quarter)]
        return remote(
            ref, ref, t1_send.at[r, e], t1_recv.at[r, e], sp=group_dev(1 if r == 3 else r)
        )

    def t2_copy(r, e, landed=False):
        ref = first.at[member(r), c, 1 - x if landed else x, pl.ds(e * quarter, quarter)]
        return remote(ref, ref, t2_send.at[r, e], t2_recv.at[r, e], tp=across)

    def t3_copy(r, h, e, landed=False):
        xh = x if h == 0 else 1 - x
        ref = first.at[member(r), 1 - c if landed else c, xh, pl.ds(e * quarter, quarter)]
        return remote(ref, ref, t3_send.at[r, h, e], t3_recv.at[r, h, e], tp=sibling)

    for e in range(2):
        for r in (2, 1):
            t1_copy(r, e).start()
    for e in range(2):
        for h in range(2):
            t3_copy(0, h, e).start()
    send_mat(1, [r for r in straight if r < half_n] + turning, False)

    @pl.when(jnp.logical_not(inner))
    def _():
        send_mat(1, far_straight, False)
        send_mat(1, far_straight, True)

    send_up(1, far_straight)

    def up_block(mm):
        def one(i, _):
            ch = i // 2
            lanes = aligned(lax.rem(i, 2) * (sub // 2), sub // 2)
            a = jnp.dot(
                first[mm, ch, 0], up[pl.ds(0, half_feat), lanes], preferred_element_type=F32
            ) + jnp.dot(
                first[mm, ch, 1],
                up[pl.ds(half_feat, half_feat), lanes],
                preferred_element_type=F32,
            )
            a = jnp.maximum(a, 0.0)
            act[aligned(mm * tok + ch * part, part), lanes] = (a * a).astype(BF16)
            return 0

        lax.fori_loop(0, 4, one, 0)

    for r, e in ((2, 0), (1, 0), (2, 1), (1, 1), (3, 0), (3, 1)):
        t1_copy(r, e, landed=True).wait_recv()
        if r == 2:
            t1_copy(3, e).start()
        t2_copy(r, e).start()
        t3_copy(r, 0, e).start()
    for e in range(2):
        for h in range(2):
            t3_copy(0, h, e, landed=True).wait_recv()
    for r in range(1, n):
        w_copy(0, r, landed=True).wait_recv()
    up_block(m)
    for r in (2, 1, 3):
        for e in range(2):
            t2_copy(r, e, landed=True).wait_recv()
            t3_copy(r, 1, e).start()
        for e in range(2):
            for h in range(2):
                t3_copy(r, h, e, landed=True).wait_recv()
        up_block(member(r))

    def piece(mm, tq, fh):
        rows = aligned((tq * (cols // block) + fh) * block, block)
        return lax.dot_general(
            act[aligned(mm * tok, tok), :],
            down[rows, :],
            (((1,), (1,)), ((), ())),
            preferred_element_type=F32,
        )

    def pair_copy(p, mm):
        return remote(
            pair_out.at[p, mm],
            pair_in.at[p, mm],
            pair_send.at[p, mm],
            pair_recv.at[p, mm],
            tp=sibling,
        )

    def near_copy(p, h, r):
        return remote(
            summed.at[p, h, member(r)],
            near_in.at[p, h, r],
            near_send.at[p, h, r],
            near_recv.at[p, h, r],
            sp=group_dev(r),
        )

    def side_copy(mm):
        return remote(side_out.at[mm], side_in.at[mm], side_send.at[mm], side_recv.at[mm], tp=across)

    def cross_copy():
        return remote(cross_out, cross_in, cross_send.at[0], cross_recv.at[0], tp=across)

    member_order = (3, 1, 2, 0)

    def reduce_phase(p):
        xp = group if p == 0 else 1 - group
        far = range(half_n, n) if p else range(1, half_n)
        for r in far:
            w_copy(1, r, landed=True).wait_recv()
        for r in member_order:
            mm = member(r)
            for fh in range(2):
                pair_out[p, mm, :, pl.ds(fh * block, block)] = piece(
                    mm, 2 * xp + 1 - c, fh
                ).astype(BF16)
            pair_copy(p, mm).start()
        for r in member_order:
            mm = member(r)
            pair_copy(p, mm).wait_recv()
            v = piece(mm, 2 * xp + c, 1) + pair_in[p, mm, :, pl.ds(block, block)].astype(F32)
            summed[p, 1, mm] = v.astype(BF16)
            if r:
                near_copy(p, 1, r).start()
            v = piece(mm, 2 * xp + c, 0) + pair_in[p, mm, :, pl.ds(0, block)].astype(F32)

            @pl.when(xp == x)
            def _():
                held[mm] = v

            @pl.when(xp != x)
            def _():
                side_out[mm] = v.astype(BF16)
                side_copy(mm).start()

    def side_phase(p):
        xp = group if p == 0 else 1 - group

        @pl.when(xp == x)
        def _():
            for r in member_order:
                mm = member(r)
                side_copy(mm).wait_recv()
                if r:
                    summed[p, 0, mm] = (held[mm] + side_in[mm].astype(F32)).astype(BF16)
                    near_copy(p, 0, r).start()

    def gather_phase(p, mine):
        xp = group if p == 0 else 1 - group

        def total(at):
            v = summed[p, 1, m, at, :].astype(F32)
            for r in range(1, GROUP):
                v = v + near_in[p, 1, r, at, :].astype(F32)
            return v

        @pl.when(xp == x if mine else xp != x)
        def _():
            for r in range(1, GROUP):
                near_copy(p, 1, r).wait_recv()
                if mine:
                    near_copy(p, 0, r).wait_recv()

            def rows(i, _):
                at = aligned(i * 64, 64)
                if mine:
                    mixed_ref[at, pl.ds(block, block)] = total(at)
                    v = held[m, at, :] + side_in[m, at, :].astype(F32)
                    for r in range(1, GROUP):
                        v = v + near_in[p, 0, r, at, :].astype(F32)
                    mixed_ref[at, pl.ds(0, block)] = v
                else:
                    cross_out[at, :] = total(at).astype(BF16)
                return 0

            lax.fori_loop(0, tok // 64, rows, 0)
            if not mine:
                cross_copy().start()

    reduce_phase(0)
    reduce_phase(1)
    side_phase(0)
    side_phase(1)
    for p in range(2):
        gather_phase(p, False)
    for p in range(2):
        gather_phase(p, True)
    cross_copy().wait_recv()

    row_tile = 128
    for i in range(tok // row_tile):
        at = pl.ds(i * row_tile, row_tile)
        ch = i // (part // row_tile)
        inner = pl.ds((i % (part // row_tile)) * row_tile, row_tile)
        v = ALPHA * first[m, ch, x, inner, lanes_of(c, cols)].astype(F32)
        v = v + jnp.concatenate(
            [
                mixed_ref[at, pl.ds(0, block)],
                mixed_ref[at, pl.ds(block, block)] + cross_in[at, :].astype(F32),
            ],
            axis=1,
        )
        mixed_ref[at, :] = v
        sums = jnp.sum(v, axis=1, keepdims=True)
        squares = jnp.sum(v * v, axis=1, keepdims=True)
        lane = lax.broadcasted_iota(jnp.int32, (row_tile, 128), 1)
        st = jnp.where(lane == 0, sums, jnp.where(lane == 1, squares, 0.0))
        stat[q, :, at] = st.T[0:8, :]

    def stat_copy(r, landed=False):
        owner = flip(q, r) if landed else q
        return remote(
            stat.at[owner], stat.at[owner], stat_send.at[r], stat_recv.at[r], tp=flip(q, r)
        )

    for r in range(1, t):
        stat_copy(r).start()

    for cp in exchange():
        cp.wait_send()
    def br_rest(slot, _):
        br_landed(slot)
        return 0

    lax.fori_loop(2 * z + 2, n, br_rest, 0)
    for r in range(1, n):
        br_copy(r).wait_send()
        w_copy(0, r).wait_send()
        w_copy(1, r).wait_send()
    for r in (1, 2):
        ow_copy(r).wait_send()
    ow_pass().wait_send()
    for r in range(1, t):
        res_copy(r).wait_send()
    for i in range(len(att_list)):
        att_copy(i).wait_send()
    for r in range(1, GROUP):
        for e in range(2):
            t1_copy(r, e).wait_send()
            t2_copy(r, e).wait_send()
        for p in range(2):
            near_copy(p, 1, r).wait_send()
        near_copy(jnp.where(group == x, 0, 1), 0, r).wait_send()
    for r in range(GROUP):
        for h in range(2):
            for e in range(2):
                t3_copy(r, h, e).wait_send()
        for p in range(2):
            pair_copy(p, r).wait_send()
        side_copy(r).wait_send()
    cross_copy().wait_send()

    for r in range(1, t):
        stat_copy(r, landed=True).wait_recv()
    for i in range(tok // row_tile):
        at = pl.ds(i * row_tile, row_tile)
        st = stat[0, :, at]
        for g in range(1, t):
            st = st + stat[g, :, at]
        st = jnp.concatenate([st, jnp.zeros((120, row_tile), F32)], axis=0).T
        center = st[:, 0:1] / feat
        spread = st[:, 1:2] / feat - center * center
        v = (mixed_ref[at, :] - center) * lax.rsqrt(spread + EPSILON)
        out_ref[at, :] = (v * g2_ref[q] + b2_ref[q]).astype(BF16)
    for r in range(1, t):
        stat_copy(r).wait_send()


def grouped_call(n, t, args):
    (
        queries,
        keys,
        values,
        breaks,
        residual_in,
        out_weight,
        first_gain,
        first_shift,
        up_weight,
        down_weight,
        second_gain,
        second_shift,
    ) = args
    tok, width = queries.shape
    heads = breaks.shape[1]
    hd = width // heads
    feat = out_weight.shape[1]
    cols = residual_in.shape[1]
    sub = up_weight.shape[1] // GROUP
    part = tok // 2
    br = jnp.pad(breaks.astype(F32).T, ((0, 8 - heads), (0, 0)))
    any_ = pl.BlockSpec(memory_space=pl.ANY)
    vmem = pl.BlockSpec(memory_space=pltpu.VMEM)
    dma = pltpu.SemaphoreType.DMA
    v = pltpu.VMEM
    return pl.pallas_call(
        functools.partial(grouped_kernel, n, t),
        out_shape=jax.ShapeDtypeStruct((tok, cols), BF16),
        in_specs=[any_] * 6 + [vmem, vmem, any_, any_, vmem, vmem],
        out_specs=vmem,
        scratch_shapes=[
            v((n, tok, 2 * hd), BF16),
            v((2, tok, hd), BF16),
            v((n, 8, tok), F32),
            v((2, tok, 128), F32),
            v((2, tok, hd), F32),
            v((2, tok, hd), BF16),
            v((t, part, width), BF16),
            v((256, 256), BF16),
            v((t, width, feat), BF16),
            v((t, part, cols), BF16),
            v((part, feat), F32),
            v((GROUP, 2, 2, part, feat // 2), BF16),
            v((feat, sub), BF16),
            v((feat, sub), BF16),
            v((GROUP * tok, sub), BF16),
            v((2, GROUP, tok, cols), BF16),
            v((2, GROUP, tok, cols), BF16),
            v((2, 2, GROUP, tok, cols // 2), BF16),
            v((2, 2, GROUP, tok, cols // 2), BF16),
            v((GROUP, tok, cols // 2), F32),
            v((GROUP, tok, cols // 2), BF16),
            v((GROUP, tok, cols // 2), BF16),
            v((tok, cols // 2), BF16),
            v((tok, cols // 2), BF16),
            v((tok, cols), F32),
            v((t, 8, tok), F32),
            dma((n,)),
            dma((n,)),
            dma((3,)),
            dma((3,)),
            dma((n,)),
            dma((n,)),
            dma((t,)),
            dma((t,)),
            dma((t,)),
            dma((t,)),
            dma((2 * t - 1,)),
            dma((2 * t - 1,)),
            dma((2, n)),
            dma((2, n)),
            dma((GROUP, 2)),
            dma((GROUP, 2)),
            dma((GROUP, 2)),
            dma((GROUP, 2)),
            dma((GROUP, 2, 2)),
            dma((GROUP, 2, 2)),
            dma((2, GROUP)),
            dma((2, GROUP)),
            dma((2, 2, GROUP)),
            dma((2, 2, GROUP)),
            dma((GROUP,)),
            dma((GROUP,)),
            dma((1,)),
            dma((1,)),
            dma((t,)),
            dma((t,)),
            dma((8,)),
            pltpu.SemaphoreType.REGULAR,
        ],
        compiler_params=pltpu.CompilerParams(
            collective_id=0, has_side_effects=True, vmem_limit_bytes=62 * 1024 * 1024
        ),
    )(
        queries,
        keys,
        values,
        br,
        residual_in,
        out_weight,
        first_gain.reshape(1, feat),
        first_shift.reshape(1, feat),
        up_weight,
        down_weight,
        second_gain.reshape(t, 1, cols),
        second_shift.reshape(t, 1, cols),
    )


def solution(mesh):
    n, t = mesh.shape["sp"], mesh.shape["tp"]

    def body(
        queries,
        keys,
        values,
        breaks,
        residual_in,
        out_weight,
        first_gain,
        first_shift,
        up_weight,
        down_weight,
        second_gain,
        second_shift,
    ):
        tok, width = queries.shape
        heads = breaks.shape[1]
        if heads == 2 and t == 4 and n == 2 * GROUP:
            return grouped_call(
                n,
                t,
                (
                    queries,
                    keys,
                    values,
                    breaks,
                    residual_in,
                    out_weight,
                    first_gain,
                    first_shift,
                    up_weight,
                    down_weight,
                    second_gain,
                    second_shift,
                ),
            )
        feat = out_weight.shape[1]
        cols = residual_in.shape[1]
        hidden = up_weight.shape[1]
        block = up_weight.shape[0]
        per = n // t
        kv = jnp.concatenate([keys, values], axis=1)
        br = jnp.pad(breaks.astype(F32).T, ((0, 8 - heads), (0, 0)))
        any_ = pl.BlockSpec(memory_space=pl.ANY)
        vmem = pl.BlockSpec(memory_space=pltpu.VMEM)
        dma = pltpu.SemaphoreType.DMA
        ring = dma((3, 2, n // 2 + 1, 2))
        return pl.pallas_call(
            functools.partial(layer_kernel, n, t, heads),
            out_shape=jax.ShapeDtypeStruct((tok, cols), BF16),
            in_specs=[vmem, any_, any_, any_, any_, vmem, vmem, any_, any_, vmem, vmem],
            out_specs=vmem,
            scratch_shapes=[
                pltpu.VMEM((n * tok, 2 * width), BF16),
                pltpu.VMEM((feat, hidden), BF16),
                pltpu.VMEM((feat, hidden), BF16),
                pltpu.VMEM((n, 8, tok), F32),
                pltpu.VMEM((t, width, feat), BF16),
                pltpu.VMEM((t, tok, cols), BF16),
                pltpu.VMEM((heads, tok, 128), F32),
                pltpu.VMEM((tok, width), F32),
                pltpu.VMEM((t, tok, width), BF16),
                pltpu.VMEM((tok, tok), BF16),
                pltpu.VMEM((tok, feat), F32),
                pltpu.VMEM((tok, feat), BF16),
                pltpu.VMEM((tok, hidden), BF16),
                pltpu.VMEM((n, tok, block), BF16),
                pltpu.VMEM((t, per, tok, block), BF16),
                pltpu.VMEM((t, 8, tok), F32),
                ring,
                ring,
                dma((n,)),
                dma((n,)),
                dma((t,)),
                dma((t,)),
                dma((t,)),
                dma((t,)),
                dma((t,)),
                dma((t,)),
                dma((n,)),
                dma((t, per)),
                dma((t,)),
                dma((t,)),
                dma((6,)),
            ],
            compiler_params=pltpu.CompilerParams(
                collective_id=0, has_side_effects=True, vmem_limit_bytes=62 * 1024 * 1024
            ),
        )(
            queries,
            kv,
            br,
            residual_in,
            out_weight,
            first_gain.reshape(1, feat),
            first_shift.reshape(1, feat),
            up_weight,
            down_weight,
            second_gain.reshape(t, 1, cols),
            second_shift.reshape(t, 1, cols),
        )

    return jax.shard_map(
        body,
        mesh=mesh,
        in_specs=(
            P("sp", "tp"),
            P("sp", "tp"),
            P("sp", "tp"),
            P("sp", "tp"),
            P("sp", "tp"),
            P("tp", None),
            P(),
            P(),
            P("sp", "tp"),
            P("sp", "tp"),
            P(),
            P(),
        ),
        out_specs=P("sp", "tp"),
        check_vma=False,
    )
```

```python
import functools

import jax
import jax.numpy as jnp
from jax import lax
from jax.experimental import pallas as pl
from jax.experimental.pallas import tpu as pltpu
from jax.sharding import PartitionSpec as P

ALPHA = 2.0**0.25
EPSILON = 1e-05
MESH = pl.DeviceIdType.MESH
F32 = jnp.float32
BF16 = jnp.bfloat16
KV, UP, DOWN = 0, 1, 2
RIGHT, LEFT = 0, 1


def aligned(start, size):
    return pl.ds(pl.multiple_of(start, size), size)


def layer_kernel(
    n,
    t,
    heads,
    q_ref,
    kv_in,
    br_in,
    res_in,
    ow_in,
    g1_ref,
    b1_ref,
    up_in,
    down_in,
    g2_ref,
    b2_ref,
    out_ref,
    kv,
    up,
    down,
    br,
    ow,
    res,
    later_sum,
    totals,
    att_all,
    lower,
    pre,
    first,
    activated,
    part,
    mix,
    stat,
    ring_send,
    ring_recv,
    br_send,
    br_recv,
    ow_send,
    ow_recv,
    res_send,
    res_recv,
    att_send,
    att_recv,
    mix_send,
    mix_recv,
    stat_send,
    stat_recv,
    local_sem,
):
    me = lax.axis_index("sp")
    me_t = lax.axis_index("tp")
    tok = q_ref.shape[0]
    width = q_ref.shape[1]
    hd = width // heads
    feat = first.shape[1]
    cols = feat // t
    block = feat // n
    per = n // t
    half_n = n // 2

    def at_pos(p):
        p = lax.rem(p + n, n)
        back = p // half_n
        return 2 * (p + back * (n - 1 - 2 * p)) + back

    pos = me // 2 + lax.rem(me, 2) * (n - 1 - 2 * (me // 2))
    next_dev = (at_pos(pos + 1), at_pos(pos - 1))
    own_in = (kv_in, up_in, down_in)
    full = (kv, up, down)
    rows_of = (tok, block, block)

    def ring_copy(item, way, hop, piece, own=False):
        rows = rows_of[item]
        half = rows // 2
        owner = at_pos(pos - (hop - 1) if way == RIGHT else pos + (hop - 1))
        dst = full[item].at[aligned(owner * rows + piece * half, half)]
        src = own_in[item].at[aligned(piece * half, half)] if own else dst
        return pltpu.make_async_remote_copy(
            src_ref=src,
            dst_ref=dst,
            send_sem=ring_send.at[item, way, hop, piece],
            recv_sem=ring_recv.at[item, way, hop, piece],
            device_id={"sp": next_dev[way]},
            device_id_type=MESH,
        )

    def ring_landed(item, way, hop, piece):
        rows = rows_of[item]
        half = rows // 2
        owner = at_pos(pos - hop if way == RIGHT else pos + hop)
        dst = full[item].at[aligned(owner * rows + piece * half, half)]
        return pltpu.make_async_remote_copy(
            src_ref=dst,
            dst_ref=dst,
            send_sem=ring_send.at[item, way, hop, piece],
            recv_sem=ring_recv.at[item, way, hop, piece],
            device_id={"sp": next_dev[way]},
            device_id_type=MESH,
        )

    def start_own(item):
        ring_copy(item, RIGHT, 1, 0, own=True).start()
        ring_copy(item, LEFT, 1, 1, own=True).start()
        ring_copy(item, RIGHT, 1, 1, own=True).start()
        ring_copy(item, LEFT, 1, 0, own=True).start()

    def event(item, e, hop=None, second=None):
        static = isinstance(e, int)
        hop = 1 + e // 2
        second = e % 2 if static else lax.rem(e, 2)
        ring_landed(item, RIGHT, hop, second).wait_recv()

        def forward_right():
            ring_copy(item, RIGHT, hop + 1, second).start()

        def forward_left():
            ring_copy(item, LEFT, hop + 1, 1 - second).start()

        def start_next():
            if item < DOWN:
                start_own(item + 1)

        def guarded(cond, fn):
            if static:
                if cond:
                    fn()
            else:
                pl.when(cond)(fn)

        guarded(e < n - 3, forward_right)
        ring_landed(item, LEFT, hop, 1 - second).wait_recv()
        guarded(e < n - 3, forward_left)
        guarded(e == n - 4, start_next)

    def drain_sends(item):
        def one(e, _):
            hop = 1 + e // 2
            second = lax.rem(e, 2)
            ring_copy(item, RIGHT, hop, second).wait_send()
            ring_copy(item, LEFT, hop, 1 - second).wait_send()
            return 0

        lax.fori_loop(0, n - 1, one, 0)

    def peer_t(d):
        return lax.rem(me_t + d, t)

    def tp_copy(src, dst_of, sends, recvs, d):
        return pltpu.make_async_remote_copy(
            src_ref=src,
            dst_ref=dst_of(me_t),
            send_sem=sends.at[d],
            recv_sem=recvs.at[d],
            device_id={"tp": peer_t(d)},
            device_id_type=MESH,
        )

    def tp_landed(dst_of, sends, recvs, d):
        dst = dst_of(lax.rem(me_t + t - d, t))
        return pltpu.make_async_remote_copy(
            src_ref=dst,
            dst_ref=dst,
            send_sem=sends.at[d],
            recv_sem=recvs.at[d],
            device_id={"tp": peer_t(d)},
            device_id_type=MESH,
        )

    def br_copy(d, landed=False):
        owner = lax.rem(me + n - d, n) if landed else me
        return pltpu.make_async_remote_copy(
            src_ref=br.at[owner] if landed else br_in,
            dst_ref=br.at[owner],
            send_sem=br_send.at[d],
            recv_sem=br_recv.at[d],
            device_id={"sp": lax.rem(me + d, n)},
            device_id_type=MESH,
        )

    barrier = pltpu.get_barrier_semaphore()

    def greet(d, _):
        pl.semaphore_signal(
            barrier, inc=1, device_id={"sp": lax.rem(me + d, n)}, device_id_type=MESH
        )
        return 0

    lax.fori_loop(1, n, greet, 0)
    for d in range(1, t):
        pl.semaphore_signal(barrier, inc=1, device_id={"tp": peer_t(d)}, device_id_type=MESH)

    res_at = lambda g: res.at[g]
    ow_at = lambda g: ow.at[g]
    att_at = lambda g: att_all.at[g]

    locals_ = [
        pltpu.make_async_copy(kv_in, kv.at[aligned(me * tok, tok)], local_sem.at[0]),
        pltpu.make_async_copy(up_in, up.at[aligned(me * block, block)], local_sem.at[1]),
        pltpu.make_async_copy(down_in, down.at[aligned(me * block, block)], local_sem.at[2]),
        pltpu.make_async_copy(br_in, br.at[me], local_sem.at[3]),
        pltpu.make_async_copy(res_in, res.at[me_t], local_sem.at[4]),
        pltpu.make_async_copy(ow_in, ow.at[me_t], local_sem.at[5]),
    ]
    pl.semaphore_wait(barrier, n - 1 + t - 1)
    start_own(KV)

    def send_breaks(d, _):
        br_copy(d).start()
        return 0

    lax.fori_loop(1, n, send_breaks, 0)
    for c in locals_:
        c.start()
    for d in range(1, t):
        tp_copy(ow_in, ow_at, ow_send, ow_recv, d).start()
    for d in range(1, t):
        tp_copy(res_in, res_at, res_send, res_recv, d).start()

    key_row = lax.broadcasted_iota(jnp.int32, (tok, tok), 0)
    key_col = lax.broadcasted_iota(jnp.int32, (tok, tok), 1)
    lower[...] = jnp.where(key_row > key_col, 1.0, 0.0).astype(BF16)
    later_sum[...] = jnp.zeros_like(later_sum)
    totals[...] = jnp.zeros_like(totals)

    def kv_event(e, _):
        event(KV, e)
        return 0

    lax.fori_loop(0, n - 2, kv_event, 0)

    def last_event(item):
        ring_landed(item, RIGHT, half_n, 0).wait_recv()
        ring_landed(item, LEFT, half_n, 1).wait_recv()

    last_event(KV)

    def wait_breaks(d, _):
        br_copy(d, landed=True).wait_recv()
        return 0

    lax.fori_loop(1, n, wait_breaks, 0)
    for c in locals_:
        c.wait()

    scale = hd ** (-0.5)
    tile = 128

    def attend_block(j):
        b = me - j
        for h in range(heads):
            def rows(i, _):
                at = aligned(i * tile, tile)
                keys = kv[aligned(b * tok, tok), pl.ds(h * hd, hd)]
                vals = kv[aligned(b * tok, tok), pl.ds(width + h * hd, hd)]
                z = lax.dot_general(
                    q_ref[at, pl.ds(h * hd, hd)],
                    keys,
                    (((1,), (1,)), ((), ())),
                    preferred_element_type=F32,
                )
                z = z * scale + br[b, pl.ds(h, 1), :]
                soft = jnp.log(1.0 + jnp.exp(-jnp.abs(z)))
                log_break = jnp.minimum(z, 0.0) - soft
                r = lax.broadcasted_iota(jnp.int32, (tile, tok), 0) + i * tile + j * tok
                strict = lax.broadcasted_iota(jnp.int32, (tile, tok), 1) < r
                log_keep = jnp.where(strict, log_break - z, 0.0)
                high = log_keep.astype(BF16)
                low = (log_keep - high.astype(F32)).astype(BF16)
                tri = lower[...]
                later = jnp.dot(high, tri, preferred_element_type=F32) + jnp.dot(
                    low, tri, preferred_element_type=F32
                )
                before = later_sum[h, at, :]
                w = jnp.exp(log_break + later + before[:, 0:1])
                w = jnp.where(strict, w, 0.0).astype(BF16)
                totals[at, pl.ds(h * hd, hd)] += jnp.dot(w, vals, preferred_element_type=F32)
                later_sum[h, at, :] = before + jnp.sum(log_keep, axis=1, keepdims=True)
                return 0

            lax.fori_loop(0, tok // tile, rows, 0)

    def attend_step(j, _):
        @pl.when(j <= me)
        def _():
            attend_block(j)

        @pl.when(j < n - 2)
        def _():
            event(UP, j)

        return 0

    lax.fori_loop(0, n, attend_step, 0)

    own_att = att_all.at[me_t]
    own_att[...] = totals[...].astype(BF16)
    for d in range(1, t):
        tp_copy(own_att, att_at, att_send, att_recv, d).start()
    last_event(UP)
    for d in range(1, t):
        tp_landed(ow_at, ow_send, ow_recv, d).wait_recv()
        tp_landed(res_at, res_send, res_recv, d).wait_recv()
    for d in range(1, t):
        tp_landed(att_at, att_send, att_recv, d).wait_recv()

    big = 256

    def mix_rows(i, _):
        at = aligned(i * big, big)
        for c in range(t):
            lanes = pl.ds(c * cols, cols)
            acc = ALPHA * res[c, at, :].astype(F32)
            mixed = jnp.zeros((big, cols), F32)
            for g in range(t):
                mixed = mixed + jnp.dot(
                    att_all[g, at, :], ow[g, :, lanes], preferred_element_type=F32
                ).astype(BF16).astype(F32)
            pre[at, lanes] = acc + mixed
        return 0

    lax.fori_loop(0, tok // big, mix_rows, 0)
    event(DOWN, 0)

    small = 64

    def norm_rows(i, _):
        at = aligned(i * small, small)
        x = pre[at, :]
        center = jnp.sum(x, axis=1, keepdims=True) / feat
        x = x - center
        spread = jnp.sum(x * x, axis=1, keepdims=True) / feat
        first[at, :] = (x * lax.rsqrt(spread + EPSILON) * g1_ref[...] + b1_ref[...]).astype(BF16)
        return 0

    lax.fori_loop(0, tok // small, norm_rows, 0)

    hidden = up.shape[1]
    strip = 256

    def up_cols(i, _):
        lanes = aligned(i * strip, strip)
        a = jnp.dot(first[...], up[:, lanes], preferred_element_type=F32)
        a = jnp.maximum(a, 0.0)
        activated[:, lanes] = (a * a).astype(BF16)
        return 0

    event(DOWN, 1)
    lax.fori_loop(0, hidden // strip, up_cols, 0)

    def mix_copy(s):
        k = lax.rem(s, per)
        owner = s // per
        return owner, pltpu.make_async_remote_copy(
            src_ref=part.at[s],
            dst_ref=mix.at[me_t, k],
            send_sem=mix_send.at[s],
            recv_sem=mix_recv.at[me_t, k],
            device_id={"tp": owner},
            device_id_type=MESH,
        )

    def down_block(s):
        y = lax.dot_general(
            activated[...],
            down[aligned(s * block, block), :],
            (((1,), (1,)), ((), ())),
            preferred_element_type=F32,
        ).astype(BF16)
        owner, copy = mix_copy(s)

        @pl.when(owner == me_t)
        def _():
            mix[me_t, lax.rem(s, per)] = y

        @pl.when(owner != me_t)
        def _():
            part[s] = y
            copy.start()

    down_block(me)

    def down_step(h, _):
        @pl.when(h > 1)
        def _():
            event(DOWN, 2 * h - 2)
            event(DOWN, 2 * h - 1)

        def side(w, _):
            down_block(at_pos(pos + (2 * w - 1) * h))
            return 0

        lax.fori_loop(0, 2, side, 0)
        return 0

    lax.fori_loop(1, half_n, down_step, 0)
    last_event(DOWN)
    down_block(at_pos(pos + half_n))

    def mix_wait(s, _):
        owner, copy = mix_copy(s)

        @pl.when(owner != me_t)
        def _():
            copy.wait_send()

        return 0

    for d in range(1, t):
        g = lax.rem(me_t + t - d, t)
        for k in range(per):
            dst = mix.at[g, k]
            pltpu.make_async_remote_copy(
                src_ref=dst,
                dst_ref=dst,
                send_sem=mix_send.at[0],
                recv_sem=mix_recv.at[g, k],
                device_id={"tp": peer_t(d)},
                device_id_type=MESH,
            ).wait_recv()

    def second_pre(i, _):
        at = aligned(i * 128, 128)
        sums = jnp.zeros((128, 1), F32)
        squares = jnp.zeros((128, 1), F32)
        x = ALPHA * first[at, aligned(me_t * cols, cols)].astype(F32)
        pieces = []
        for k in range(per):
            v = mix[0, k, at, :].astype(F32)
            for g in range(1, t):
                v = v + mix[g, k, at, :].astype(F32)
            pieces.append(v)
        x = x + (jnp.concatenate(pieces, axis=1) if per > 1 else pieces[0])
        pre[at, pl.ds(0, cols)] = x
        sums = jnp.sum(x, axis=1, keepdims=True)
        squares = jnp.sum(x * x, axis=1, keepdims=True)
        lane = lax.broadcasted_iota(jnp.int32, (128, 128), 1)
        s = jnp.where(lane == 0, sums, jnp.where(lane == 1, squares, 0.0))
        stat[me_t, :, at] = s.T[0:8, :]
        return 0

    for i in range(tok // 128):
        second_pre(i, 0)
    stat_at = lambda g: stat.at[g]
    for d in range(1, t):
        tp_copy(stat.at[me_t], stat_at, stat_send, stat_recv, d).start()

    lax.fori_loop(0, n, mix_wait, 0)
    for item in (KV, UP, DOWN):
        drain_sends(item)

    def br_done(d, _):
        br_copy(d).wait_send()
        return 0

    lax.fori_loop(1, n, br_done, 0)
    for d in range(1, t):
        tp_copy(ow_in, ow_at, ow_send, ow_recv, d).wait_send()
        tp_copy(res_in, res_at, res_send, res_recv, d).wait_send()
        tp_copy(own_att, att_at, att_send, att_recv, d).wait_send()
    for d in range(1, t):
        tp_landed(stat_at, stat_send, stat_recv, d).wait_recv()

    for i in range(tok // 128):
        at = pl.ds(i * 128, 128)
        s = stat[0, :, at]
        for g in range(1, t):
            s = s + stat[g, :, at]
        s = jnp.concatenate([s, jnp.zeros((120, 128), F32)], axis=0).T
        center = s[:, 0:1] / feat
        spread = s[:, 1:2] / feat - center * center
        x = pre[at, pl.ds(0, cols)]
        x = (x - center) * lax.rsqrt(spread + EPSILON)
        out_ref[at, :] = (x * g2_ref[me_t] + b2_ref[me_t]).astype(BF16)
    for d in range(1, t):
        tp_copy(stat.at[me_t], stat_at, stat_send, stat_recv, d).wait_send()


GROUP = 4


def flip(a, r):
    bit = 1
    out = a
    while bit <= r:
        if r & bit:
            out = out + bit - 2 * bit * lax.rem(a // bit, 2)
        bit *= 2
    return out


def remote(src, dst, send, recv, **where):
    return pltpu.make_async_remote_copy(
        src_ref=src,
        dst_ref=dst,
        send_sem=send,
        recv_sem=recv,
        device_id=where,
        device_id_type=MESH,
    )


def grouped_kernel(
    n,
    t,
    q_in,
    k_in,
    v_in,
    br_in,
    res_in,
    ow_in,
    g1_ref,
    b1_ref,
    up_in,
    down_in,
    g2_ref,
    b2_ref,
    out_ref,
    kvb,
    qb,
    br,
    later_sum,
    totals,
    att_own,
    att_all,
    tri_ref,
    ow,
    res,
    pre,
    first,
    up,
    down,
    act,
    pair_out,
    pair_in,
    summed,
    near_in,
    held,
    side_out,
    side_in,
    cross_out,
    cross_in,
    mixed_ref,
    stat,
    kv_send,
    kv_recv,
    kx_send,
    kx_recv,
    br_send,
    br_recv,
    ow_send,
    ow_recv,
    res_send,
    res_recv,
    att_send,
    att_recv,
    w_send,
    w_recv,
    t1_send,
    t1_recv,
    t2_send,
    t2_recv,
    t3_send,
    t3_recv,
    pair_send,
    pair_recv,
    near_send,
    near_recv,
    side_send,
    side_recv,
    cross_send,
    cross_recv,
    stat_send,
    stat_recv,
    local_sem,
    go_sem,
    pair_sem,
):
    s = lax.axis_index("sp")
    q = lax.axis_index("tp")
    y = lax.rem(s, 2)
    z = s // 2
    levels = n // 2
    m = lax.rem(s, GROUP)
    group = s // GROUP
    x = q // 2
    c = lax.rem(q, 2)
    tok, width = q_in.shape
    hd = width // 2
    feat = ow.shape[2]
    cols = feat // t
    half_feat = feat // 2
    block = up_in.shape[0]
    sub = up_in.shape[1] // GROUP
    part = tok // 2
    half_n = n // 2
    sibling = flip(q, 1)
    across = flip(q, 2)

    barrier = pltpu.get_barrier_semaphore()
    for r in range(1, n):
        pl.semaphore_signal(barrier, inc=1, device_id={"sp": flip(s, r)}, device_id_type=MESH)
    for r in range(1, t):
        pl.semaphore_signal(barrier, inc=1, device_id={"tp": flip(q, r)}, device_id_type=MESH)
        pl.semaphore_signal(
            barrier, inc=1, device_id={"sp": flip(s, 1), "tp": flip(q, r)}, device_id_type=MESH
        )

    def lanes_of(i, size):
        return aligned(i * size, size)

    own_copies = [
        pltpu.make_async_copy(
            k_in.at[:, lanes_of(y, hd)], kvb.at[s, :, pl.ds(0, hd)], local_sem.at[0]
        ),
        pltpu.make_async_copy(
            v_in.at[:, lanes_of(y, hd)], kvb.at[s, :, pl.ds(hd, hd)], local_sem.at[1]
        ),
        pltpu.make_async_copy(q_in.at[:, lanes_of(y, hd)], qb.at[y], local_sem.at[2]),
    ]
    other_copies = [
        pltpu.make_async_copy(br_in, br.at[s], local_sem.at[3]),
        pltpu.make_async_copy(res_in.at[lanes_of(c, part)], res.at[q], local_sem.at[4]),
        pltpu.make_async_copy(ow_in, ow.at[q], local_sem.at[5]),
        pltpu.make_async_copy(
            up_in.at[:, lanes_of(m, sub)], up.at[lanes_of(s, block)], local_sem.at[6]
        ),
        pltpu.make_async_copy(
            down_in.at[:, lanes_of(m, sub)], down.at[lanes_of(s, block)], local_sem.at[7]
        ),
    ]
    for cp in own_copies:
        cp.start()

    ps = flip(s, 1)
    py = 1 - y

    def exchange(landed=False):
        own = ps if landed else s
        row = y if landed else py
        mine = py if landed else y
        return [
            remote(
                kvb.at[own, :, pl.ds(0, hd)] if landed else k_in.at[:, lanes_of(row, hd)],
                kvb.at[own, :, pl.ds(0, hd)],
                kx_send.at[0],
                kx_recv.at[0],
                sp=ps,
            ),
            remote(
                kvb.at[own, :, pl.ds(hd, hd)] if landed else v_in.at[:, lanes_of(row, hd)],
                kvb.at[own, :, pl.ds(hd, hd)],
                kx_send.at[1],
                kx_recv.at[1],
                sp=ps,
            ),
            remote(
                qb.at[mine] if landed else q_in.at[:, lanes_of(row, hd)],
                qb.at[mine],
                kx_send.at[2],
                kx_recv.at[2],
                sp=ps,
            ),
        ]

    def relay(slot):
        return remote(kvb.at[slot], kvb.at[slot], kv_send.at[slot], kv_recv.at[slot], sp=s + 2)

    def relay_landed(slot):
        return remote(kvb.at[slot], kvb.at[slot], kv_send.at[slot], kv_recv.at[slot], sp=s)

    def br_copy(r, landed=False):
        owner = flip(s, r) if landed else s
        return remote(
            br.at[owner] if landed else br_in,
            br.at[owner],
            br_send.at[r],
            br_recv.at[owner],
            sp=flip(s, r),
        )

    def ow_copy(r, landed=False):
        owner = flip(q, r) if landed else q
        return remote(
            ow.at[owner] if landed else ow_in,
            ow.at[owner],
            ow_send.at[r],
            ow_recv.at[r],
            tp=flip(q, r),
        )

    def ow_pass(landed=False):
        ref = ow.at[flip(q, 3) if landed else across]
        return remote(ref, ref, ow_send.at[3], ow_recv.at[3], tp=sibling)

    def res_copy(r, landed=False):
        to = flip(q, r)
        owner = to if landed else q
        return remote(
            res.at[owner] if landed else res_in.at[lanes_of(lax.rem(to, 2), part)],
            res.at[owner],
            res_send.at[r],
            res_recv.at[r],
            tp=to,
        )

    mats_in = (up_in, down_in)
    mats = (up, down)

    def w_copy(mat, r, landed=False):
        to = flip(s, r)
        owner = to if landed else s
        dst = mats[mat].at[lanes_of(owner, block)]
        return remote(
            dst if landed else mats_in[mat].at[:, lanes_of(lax.rem(to, GROUP), sub)],
            dst,
            w_send.at[mat, r],
            w_recv.at[mat, r],
            sp=to,
        )

    def climbs(r):
        return lax.rem(s // (half_n if r >= half_n else 2), 2) == 0

    def send_mat(mat, rs, upward):
        for r in rs:

            def go(r=r):
                w_copy(mat, r).start()

            if r < 2:
                go()
            else:
                pl.when(climbs(r) if upward else jnp.logical_not(climbs(r)))(go)

    def send_up(mat, skip=()):
        far_level = [r for r in range(half_n, n) if (r // 2) % 2 and r not in skip]
        same_level = [r for r in range(half_n, n) if not (r // 2) % 2 and r not in skip]

        @pl.when(group == 0)
        def _():
            @pl.when(lax.rem(z, 2) == 0)
            def _():
                for r in same_level + far_level:
                    w_copy(mat, r).start()

            @pl.when(lax.rem(z, 2) == 1)
            def _():
                for r in far_level + same_level:
                    w_copy(mat, r).start()

    straight = [r for r in range(n - 1, 0, -1) if r % 2 == 0]
    turning = [r for r in range(n - 1, 0, -1) if r % 2]

    pl.semaphore_wait(barrier, n - 1 + 2 * (t - 1))
    for cp in exchange():
        cp.start()
    for r in range(1, n):
        br_copy(r).start()
    for cp in other_copies:
        cp.start()
    for cp in own_copies:
        cp.wait()

    @pl.when(z < levels - 1)
    def _():
        relay(s).start()

    for r in range(1, t):
        res_copy(r).start()
    for r in (1, 2):
        ow_copy(r).start()
    send_mat(0, straight, False)

    inner = lax.rem(z, 2) != group
    far_straight = [r for r in straight if r >= half_n]

    key_row = lax.broadcasted_iota(jnp.int32, tri_ref.shape, 0)
    key_col = lax.broadcasted_iota(jnp.int32, tri_ref.shape, 1)
    tri_ref[...] = jnp.where(key_row > key_col, 1.0, 0.0).astype(BF16)
    later_sum[...] = jnp.zeros_like(later_sum)
    totals[...] = jnp.zeros_like(totals)

    for cp in other_copies:
        cp.wait()

    def br_landed(slot):
        remote(br.at[slot], br.at[slot], br_send.at[0], br_recv.at[slot], sp=s).wait_recv()

    scale = hd ** (-0.5)
    tile = 512
    span = tri_ref.shape[0]

    def attend(slot, qy, masked):
        def rows(i, _):
            at = aligned(i * tile, tile)
            z_ = lax.dot_general(
                qb[qy, at, :],
                kvb[slot, :, pl.ds(0, hd)],
                (((1,), (1,)), ((), ())),
                preferred_element_type=F32,
            )
            z_ = z_ * scale + br[slot, pl.ds(y, 1), :]
            soft = jnp.log(1.0 + jnp.exp(-jnp.abs(z_)))
            log_break = jnp.minimum(z_, 0.0) - soft
            keep = log_break - z_
            if masked:
                r = lax.broadcasted_iota(jnp.int32, (tile, tok), 0) + i * tile
                strict = lax.broadcasted_iota(jnp.int32, (tile, tok), 1) < r
                keep = jnp.where(strict, keep, 0.0)
            high = keep.astype(BF16)
            low = (keep - high.astype(F32)).astype(BF16)
            tri = tri_ref[...]
            run = later_sum[qy, at, :][:, 0:1]
            pieces = []
            for b in range(tok // span - 1, -1, -1):
                sl = slice(b * span, (b + 1) * span)
                later = jnp.dot(high[:, sl], tri, preferred_element_type=F32) + jnp.dot(
                    low[:, sl], tri, preferred_element_type=F32
                )
                pieces.append(later + run)
                run = run + jnp.sum(keep[:, sl], axis=1, keepdims=True)
            w = jnp.exp(log_break + jnp.concatenate(pieces[::-1], axis=1))
            if masked:
                w = jnp.where(strict, w, 0.0)
            totals[qy, at, :] += jnp.dot(
                w.astype(BF16), kvb[slot, :, pl.ds(hd, hd)], preferred_element_type=F32
            )
            later_sum[qy, at, :] = jnp.broadcast_to(run, (tile, 128))
            return 0

        lax.fori_loop(0, tok // tile, rows, 0)

    attend(s, y, True)
    for cp in exchange(landed=True):
        cp.wait_recv()

    @pl.when(z < levels - 1)
    def _():
        relay(ps).start()

    br_landed(ps)
    send_mat(0, turning, False)
    attend(ps, py, True)

    def fetch(slot):
        @pl.when(slot >= 0)
        def _():
            relay_landed(slot).wait_recv()
            br_landed(slot)

            @pl.when(z < levels - 1)
            def _():
                relay(slot).start()

    ahead = jnp.where(z < levels - 1, 2, 0)

    @pl.when(z < levels - 1)
    def _():
        fetch(2 * z - 1)

    attend(2 * z, 1, False)

    @pl.when(z < levels - 1)
    def _():
        fetch(2 * z - 2)

    def attend_step(k, _):
        slot = 2 * z + 1 - k
        fetch(slot - ahead)

        @pl.when(slot >= 0)
        def _():
            def one(qy, _):
                attend(slot, qy, False)
                return 0

            lax.fori_loop(0, 2, one, 0)

        return 0

    lax.fori_loop(2, n, attend_step, 0)

    @pl.when(z < levels - 1)
    def _():
        def drain(slot, _):
            relay(slot).wait_send()
            return 0

        lax.fori_loop(0, 2 * z + 2, drain, 0)
        pl.semaphore_signal(pair_sem, inc=1, device_id={"tp": sibling}, device_id_type=MESH)
        pl.semaphore_wait(pair_sem, 1)

    send_mat(0, (2, 3), True)

    @pl.when(z == 1)
    def _():
        pl.semaphore_signal(go_sem, inc=1, device_id={"sp": s - 2}, device_id_type=MESH)

    @pl.when(z == 0)
    def _():
        pl.semaphore_wait(go_sem, 1)

    send_up(0)

    @pl.when(inner)
    def _():
        send_mat(1, far_straight, False)
        send_mat(1, far_straight, True)

    ow_copy(2, landed=True).wait_recv()
    ow_pass().start()

    att_own[...] = totals[...].astype(BF16)
    att_list = [(dy, r) for dy in range(2) for r in range(t) if dy or r]

    def att_copy(i, landed=False):
        dy, r = att_list[i]
        ty = flip(y, 1) if dy else y
        tq = flip(q, r)
        sp = ps if dy else s
        if landed:
            dst = att_all.at[tq, :, lanes_of(ty, hd)]
            return remote(dst, dst, att_send.at[i], att_recv.at[i], sp=sp, tp=tq)
        return remote(
            att_own.at[ty, lanes_of(lax.rem(tq, 2), part)],
            att_all.at[q, :, lanes_of(y, hd)],
            att_send.at[i],
            att_recv.at[i],
            sp=sp,
            tp=tq,
        )

    for i in range(len(att_list)):
        att_copy(i).start()
    att_all[q, :, lanes_of(y, hd)] = att_own[y, lanes_of(c, part), :]
    ow_copy(1, landed=True).wait_recv()
    ow_pass(landed=True).wait_recv()
    for r in range(1, t):
        res_copy(r, landed=True).wait_recv()
    for i in range(len(att_list)):
        att_copy(i, landed=True).wait_recv()

    for cc in range(t):
        lanes = pl.ds(cc * cols, cols)
        mixed = jnp.zeros((part, cols), F32)
        for g in range(t):
            mixed = mixed + jnp.dot(
                att_all[g], ow[g, :, lanes], preferred_element_type=F32
            ).astype(BF16).astype(F32)
        pre[:, lanes] = ALPHA * res[cc].astype(F32) + mixed

    small = 64

    def norm_rows(i, _):
        at = aligned(i * small, small)
        v = pre[at, :]
        center = jnp.sum(v, axis=1, keepdims=True) / feat
        v = v - center
        spread = jnp.sum(v * v, axis=1, keepdims=True) / feat
        v = (v * lax.rsqrt(spread + EPSILON) * g1_ref[...] + b1_ref[...]).astype(BF16)
        first[m, c, 0, at, :] = v[:, :half_feat]
        first[m, c, 1, at, :] = v[:, half_feat:]
        return 0

    lax.fori_loop(0, part // small, norm_rows, 0)

    def member(r):
        return flip(m, r)

    def group_dev(r):
        return flip(s, r)

    quarter = part // 2

    def t1_copy(r, e, landed=False):
        owner = member(r) if landed else (member(2) if r == 3 else m)
        ref = first.at[owner, c, x, pl.ds(e * quarter, quarter)]
        return remote(
            ref, ref, t1_send.at[r, e], t1_recv.at[r, e], sp=group_dev(1 if r == 3 else r)
        )

    def t2_copy(r, e, landed=False):
        ref = first.at[member(r), c, 1 - x if landed else x, pl.ds(e * quarter, quarter)]
        return remote(ref, ref, t2_send.at[r, e], t2_recv.at[r, e], tp=across)

    def t3_copy(r, h, e, landed=False):
        xh = x if h == 0 else 1 - x
        ref = first.at[member(r), 1 - c if landed else c, xh, pl.ds(e * quarter, quarter)]
        return remote(ref, ref, t3_send.at[r, h, e], t3_recv.at[r, h, e], tp=sibling)

    for e in range(2):
        for r in (2, 1):
            t1_copy(r, e).start()
    for e in range(2):
        for h in range(2):
            t3_copy(0, h, e).start()
    send_mat(1, [r for r in straight if r < half_n], False)

    @pl.when(jnp.logical_not(inner))
    def _():
        send_mat(1, far_straight, False)
        send_mat(1, far_straight, True)

    send_mat(1, (2,), True)

    def up_block(mm):
        def one(i, _):
            ch = i // 2
            lanes = aligned(lax.rem(i, 2) * (sub // 2), sub // 2)
            a = jnp.dot(
                first[mm, ch, 0], up[pl.ds(0, half_feat), lanes], preferred_element_type=F32
            ) + jnp.dot(
                first[mm, ch, 1],
                up[pl.ds(half_feat, half_feat), lanes],
                preferred_element_type=F32,
            )
            a = jnp.maximum(a, 0.0)
            act[aligned(mm * tok + ch * part, part), lanes] = (a * a).astype(BF16)
            return 0

        lax.fori_loop(0, 4, one, 0)

    def pass_on(steps):
        for r, e in steps:
            t1_copy(r, e, landed=True).wait_recv()
            if r == 2:
                t1_copy(3, e).start()
            t2_copy(r, e).start()
            t3_copy(r, 0, e).start()

    pass_on(((1, 0), (2, 0), (1, 1), (2, 1)))
    send_mat(1, [r for r in turning if r > 1], False)
    send_mat(1, (1,), False)
    send_mat(1, (3,), True)
    send_up(1, far_straight)
    for e in range(2):
        for h in range(2):
            t3_copy(0, h, e, landed=True).wait_recv()
    for r in range(1, n):
        w_copy(0, r, landed=True).wait_recv()
    up_block(m)
    pass_on(((3, 0), (3, 1)))
    for r in (1, 2, 3):
        for e in range(2):
            t2_copy(r, e, landed=True).wait_recv()
            t3_copy(r, 1, e).start()
        for e in range(2):
            for h in range(2):
                t3_copy(r, h, e, landed=True).wait_recv()
        up_block(member(r))

    def piece(mm, tq, fh):
        rows = aligned((tq * (cols // block) + fh) * block, block)
        return lax.dot_general(
            act[aligned(mm * tok, tok), :],
            down[rows, :],
            (((1,), (1,)), ((), ())),
            preferred_element_type=F32,
        )

    def pair_copy(p, mm):
        return remote(
            pair_out.at[p, mm],
            pair_in.at[p, mm],
            pair_send.at[p, mm],
            pair_recv.at[p, mm],
            tp=sibling,
        )

    def near_copy(p, h, r):
        return remote(
            summed.at[p, h, member(r)],
            near_in.at[p, h, r],
            near_send.at[p, h, r],
            near_recv.at[p, h, r],
            sp=group_dev(2 if r == 2 else 1),
        )

    def near_on(p, h):
        near_copy(p, h, 3).wait_recv()
        both = summed[p, h, member(2)].astype(F32) + near_in[p, h, 3].astype(F32)
        summed[p, h, member(2)] = both.astype(BF16)
        near_copy(p, h, 2).start()

    def side_copy(mm):
        return remote(side_out.at[mm], side_in.at[mm], side_send.at[mm], side_recv.at[mm], tp=across)

    def cross_copy():
        return remote(cross_out, cross_in, cross_send.at[0], cross_recv.at[0], tp=across)

    member_order = (3, 1, 2, 0)

    def reduce_phase(p):
        xp = group if p == 0 else 1 - group
        far = range(half_n, n) if p else range(1, half_n)
        for r in far:
            w_copy(1, r, landed=True).wait_recv()
        for r in member_order:
            mm = member(r)
            for fh in range(2):
                pair_out[p, mm, :, pl.ds(fh * block, block)] = piece(
                    mm, 2 * xp + 1 - c, fh
                ).astype(BF16)
            pair_copy(p, mm).start()
        for r in member_order:
            mm = member(r)
            pair_copy(p, mm).wait_recv()
            v = piece(mm, 2 * xp + c, 1) + pair_in[p, mm, :, pl.ds(block, block)].astype(F32)
            summed[p, 1, mm] = v.astype(BF16)
            if r % 2:
                near_copy(p, 1, r).start()
            v = piece(mm, 2 * xp + c, 0) + pair_in[p, mm, :, pl.ds(0, block)].astype(F32)

            @pl.when(xp == x)
            def _():
                held[p, mm] = v

            @pl.when(xp != x)
            def _():
                side_out[mm] = v.astype(BF16)
                side_copy(mm).start()

    def side_phase(p, rs):
        xp = group if p == 0 else 1 - group

        @pl.when(xp == x)
        def _():
            for r in rs:
                mm = member(r)
                side_copy(mm).wait_recv()
                if r:
                    summed[p, 0, mm] = (held[p, mm] + side_in[mm].astype(F32)).astype(BF16)
                if r % 2:
                    near_copy(p, 0, r).start()
            if 0 in rs:
                near_on(p, 0)

    def gather_phase(p, mine):
        xp = group if p == 0 else 1 - group

        def total(at):
            v = summed[p, 1, m, at, :].astype(F32)
            for r in (1, 2):
                v = v + near_in[p, 1, r, at, :].astype(F32)
            return v

        @pl.when(xp == x if mine else xp != x)
        def _():
            for r in (1, 2):
                near_copy(p, 1, r).wait_recv()
                if mine:
                    near_copy(p, 0, r).wait_recv()

            def rows(i, _):
                at = aligned(i * 64, 64)
                if mine:
                    mixed_ref[at, pl.ds(block, block)] = total(at)
                    v = held[p, m, at, :] + side_in[m, at, :].astype(F32)
                    for r in (1, 2):
                        v = v + near_in[p, 0, r, at, :].astype(F32)
                    mixed_ref[at, pl.ds(0, block)] = v
                else:
                    cross_out[at, :] = total(at).astype(BF16)
                return 0

            lax.fori_loop(0, tok // 64, rows, 0)
            if not mine:
                cross_copy().start()

    reduce_phase(0)
    reduce_phase(1)
    near_on(0, 1)
    for p in range(2):
        side_phase(p, member_order[:2])
    gather_phase(0, False)
    near_on(1, 1)
    for p in range(2):
        side_phase(p, member_order[2:])
    gather_phase(1, False)
    for p in range(2):
        gather_phase(p, True)
    cross_copy().wait_recv()

    row_tile = 128
    for i in range(tok // row_tile):
        at = pl.ds(i * row_tile, row_tile)
        ch = i // (part // row_tile)
        inner = pl.ds((i % (part // row_tile)) * row_tile, row_tile)
        v = ALPHA * first[m, ch, x, inner, lanes_of(c, cols)].astype(F32)
        v = v + jnp.concatenate(
            [
                mixed_ref[at, pl.ds(0, block)],
                mixed_ref[at, pl.ds(block, block)] + cross_in[at, :].astype(F32),
            ],
            axis=1,
        )
        mixed_ref[at, :] = v
        sums = jnp.sum(v, axis=1, keepdims=True)
        squares = jnp.sum(v * v, axis=1, keepdims=True)
        lane = lax.broadcasted_iota(jnp.int32, (row_tile, 128), 1)
        st = jnp.where(lane == 0, sums, jnp.where(lane == 1, squares, 0.0))
        stat[q, :, at] = st.T[0:8, :]

    def stat_copy(r, landed=False):
        owner = flip(q, r) if landed else q
        return remote(
            stat.at[owner], stat.at[owner], stat_send.at[r], stat_recv.at[r], tp=flip(q, r)
        )

    for r in range(1, t):
        stat_copy(r).start()

    for cp in exchange():
        cp.wait_send()
    def br_rest(slot, _):
        br_landed(slot)
        return 0

    lax.fori_loop(2 * z + 2, n, br_rest, 0)
    for r in range(1, n):
        br_copy(r).wait_send()
        w_copy(0, r).wait_send()
        w_copy(1, r).wait_send()
    for r in (1, 2):
        ow_copy(r).wait_send()
    ow_pass().wait_send()
    for r in range(1, t):
        res_copy(r).wait_send()
    for i in range(len(att_list)):
        att_copy(i).wait_send()
    for r in range(1, GROUP):
        for e in range(2):
            t1_copy(r, e).wait_send()
            t2_copy(r, e).wait_send()
        for p in range(2):
            near_copy(p, 1, r).wait_send()
        near_copy(jnp.where(group == x, 0, 1), 0, r).wait_send()
    for r in range(GROUP):
        for h in range(2):
            for e in range(2):
                t3_copy(r, h, e).wait_send()
        for p in range(2):
            pair_copy(p, r).wait_send()
        side_copy(r).wait_send()
    cross_copy().wait_send()

    for r in range(1, t):
        stat_copy(r, landed=True).wait_recv()
    for i in range(tok // row_tile):
        at = pl.ds(i * row_tile, row_tile)
        st = stat[0, :, at]
        for g in range(1, t):
            st = st + stat[g, :, at]
        st = jnp.concatenate([st, jnp.zeros((120, row_tile), F32)], axis=0).T
        center = st[:, 0:1] / feat
        spread = st[:, 1:2] / feat - center * center
        v = (mixed_ref[at, :] - center) * lax.rsqrt(spread + EPSILON)
        out_ref[at, :] = (v * g2_ref[q] + b2_ref[q]).astype(BF16)
    for r in range(1, t):
        stat_copy(r).wait_send()


def grouped_call(n, t, args):
    (
        queries,
        keys,
        values,
        breaks,
        residual_in,
        out_weight,
        first_gain,
        first_shift,
        up_weight,
        down_weight,
        second_gain,
        second_shift,
    ) = args
    tok, width = queries.shape
    heads = breaks.shape[1]
    hd = width // heads
    feat = out_weight.shape[1]
    cols = residual_in.shape[1]
    sub = up_weight.shape[1] // GROUP
    part = tok // 2
    br = jnp.pad(breaks.astype(F32).T, ((0, 8 - heads), (0, 0)))
    any_ = pl.BlockSpec(memory_space=pl.ANY)
    vmem = pl.BlockSpec(memory_space=pltpu.VMEM)
    dma = pltpu.SemaphoreType.DMA
    v = pltpu.VMEM
    return pl.pallas_call(
        functools.partial(grouped_kernel, n, t),
        out_shape=jax.ShapeDtypeStruct((tok, cols), BF16),
        in_specs=[any_] * 6 + [vmem, vmem, any_, any_, vmem, vmem],
        out_specs=vmem,
        scratch_shapes=[
            v((n, tok, 2 * hd), BF16),
            v((2, tok, hd), BF16),
            v((n, 8, tok), F32),
            v((2, tok, 128), F32),
            v((2, tok, hd), F32),
            v((2, tok, hd), BF16),
            v((t, part, width), BF16),
            v((256, 256), BF16),
            v((t, width, feat), BF16),
            v((t, part, cols), BF16),
            v((part, feat), F32),
            v((GROUP, 2, 2, part, feat // 2), BF16),
            v((feat, sub), BF16),
            v((feat, sub), BF16),
            v((GROUP * tok, sub), BF16),
            v((2, GROUP, tok, cols), BF16),
            v((2, GROUP, tok, cols), BF16),
            v((2, 2, GROUP, tok, cols // 2), BF16),
            v((2, 2, GROUP, tok, cols // 2), BF16),
            v((2, GROUP, tok, cols // 2), F32),
            v((GROUP, tok, cols // 2), BF16),
            v((GROUP, tok, cols // 2), BF16),
            v((tok, cols // 2), BF16),
            v((tok, cols // 2), BF16),
            v((tok, cols), F32),
            v((t, 8, tok), F32),
            dma((n,)),
            dma((n,)),
            dma((3,)),
            dma((3,)),
            dma((n,)),
            dma((n,)),
            dma((t,)),
            dma((t,)),
            dma((t,)),
            dma((t,)),
            dma((2 * t - 1,)),
            dma((2 * t - 1,)),
            dma((2, n)),
            dma((2, n)),
            dma((GROUP, 2)),
            dma((GROUP, 2)),
            dma((GROUP, 2)),
            dma((GROUP, 2)),
            dma((GROUP, 2, 2)),
            dma((GROUP, 2, 2)),
            dma((2, GROUP)),
            dma((2, GROUP)),
            dma((2, 2, GROUP)),
            dma((2, 2, GROUP)),
            dma((GROUP,)),
            dma((GROUP,)),
            dma((1,)),
            dma((1,)),
            dma((t,)),
            dma((t,)),
            dma((8,)),
            pltpu.SemaphoreType.REGULAR,
            pltpu.SemaphoreType.REGULAR,
        ],
        compiler_params=pltpu.CompilerParams(
            collective_id=0, has_side_effects=True, vmem_limit_bytes=62 * 1024 * 1024
        ),
    )(
        queries,
        keys,
        values,
        br,
        residual_in,
        out_weight,
        first_gain.reshape(1, feat),
        first_shift.reshape(1, feat),
        up_weight,
        down_weight,
        second_gain.reshape(t, 1, cols),
        second_shift.reshape(t, 1, cols),
    )


def solution(mesh):
    n, t = mesh.shape["sp"], mesh.shape["tp"]

    def body(
        queries,
        keys,
        values,
        breaks,
        residual_in,
        out_weight,
        first_gain,
        first_shift,
        up_weight,
        down_weight,
        second_gain,
        second_shift,
    ):
        tok, width = queries.shape
        heads = breaks.shape[1]
        if heads == 2 and t == 4 and n == 2 * GROUP:
            return grouped_call(
                n,
                t,
                (
                    queries,
                    keys,
                    values,
                    breaks,
                    residual_in,
                    out_weight,
                    first_gain,
                    first_shift,
                    up_weight,
                    down_weight,
                    second_gain,
                    second_shift,
                ),
            )
        feat = out_weight.shape[1]
        cols = residual_in.shape[1]
        hidden = up_weight.shape[1]
        block = up_weight.shape[0]
        per = n // t
        kv = jnp.concatenate([keys, values], axis=1)
        br = jnp.pad(breaks.astype(F32).T, ((0, 8 - heads), (0, 0)))
        any_ = pl.BlockSpec(memory_space=pl.ANY)
        vmem = pl.BlockSpec(memory_space=pltpu.VMEM)
        dma = pltpu.SemaphoreType.DMA
        ring = dma((3, 2, n // 2 + 1, 2))
        return pl.pallas_call(
            functools.partial(layer_kernel, n, t, heads),
            out_shape=jax.ShapeDtypeStruct((tok, cols), BF16),
            in_specs=[vmem, any_, any_, any_, any_, vmem, vmem, any_, any_, vmem, vmem],
            out_specs=vmem,
            scratch_shapes=[
                pltpu.VMEM((n * tok, 2 * width), BF16),
                pltpu.VMEM((feat, hidden), BF16),
                pltpu.VMEM((feat, hidden), BF16),
                pltpu.VMEM((n, 8, tok), F32),
                pltpu.VMEM((t, width, feat), BF16),
                pltpu.VMEM((t, tok, cols), BF16),
                pltpu.VMEM((heads, tok, 128), F32),
                pltpu.VMEM((tok, width), F32),
                pltpu.VMEM((t, tok, width), BF16),
                pltpu.VMEM((tok, tok), BF16),
                pltpu.VMEM((tok, feat), F32),
                pltpu.VMEM((tok, feat), BF16),
                pltpu.VMEM((tok, hidden), BF16),
                pltpu.VMEM((n, tok, block), BF16),
                pltpu.VMEM((t, per, tok, block), BF16),
                pltpu.VMEM((t, 8, tok), F32),
                ring,
                ring,
                dma((n,)),
                dma((n,)),
                dma((t,)),
                dma((t,)),
                dma((t,)),
                dma((t,)),
                dma((t,)),
                dma((t,)),
                dma((n,)),
                dma((t, per)),
                dma((t,)),
                dma((t,)),
                dma((6,)),
            ],
            compiler_params=pltpu.CompilerParams(
                collective_id=0, has_side_effects=True, vmem_limit_bytes=62 * 1024 * 1024
            ),
        )(
            queries,
            kv,
            br,
            residual_in,
            out_weight,
            first_gain.reshape(1, feat),
            first_shift.reshape(1, feat),
            up_weight,
            down_weight,
            second_gain.reshape(t, 1, cols),
            second_shift.reshape(t, 1, cols),
        )

    return jax.shard_map(
        body,
        mesh=mesh,
        in_specs=(
            P("sp", "tp"),
            P("sp", "tp"),
            P("sp", "tp"),
            P("sp", "tp"),
            P("sp", "tp"),
            P("tp", None),
            P(),
            P(),
            P("sp", "tp"),
            P("sp", "tp"),
            P(),
            P(),
        ),
        out_specs=P("sp", "tp"),
        check_vma=False,
    )
```

```python
import functools

import jax
import jax.numpy as jnp
from jax import lax
from jax.experimental import pallas as pl
from jax.experimental.pallas import tpu as pltpu
from jax.sharding import PartitionSpec as P

ALPHA = 2.0**0.25
EPSILON = 1e-05
MESH = pl.DeviceIdType.MESH
F32 = jnp.float32
BF16 = jnp.bfloat16
KV, UP, DOWN = 0, 1, 2
RIGHT, LEFT = 0, 1


def aligned(start, size):
    return pl.ds(pl.multiple_of(start, size), size)


def layer_kernel(
    n,
    t,
    heads,
    q_ref,
    kv_in,
    br_in,
    res_in,
    ow_in,
    g1_ref,
    b1_ref,
    up_in,
    down_in,
    g2_ref,
    b2_ref,
    out_ref,
    kv,
    up,
    down,
    br,
    ow,
    res,
    later_sum,
    totals,
    att_all,
    lower,
    pre,
    first,
    activated,
    part,
    mix,
    stat,
    ring_send,
    ring_recv,
    br_send,
    br_recv,
    ow_send,
    ow_recv,
    res_send,
    res_recv,
    att_send,
    att_recv,
    mix_send,
    mix_recv,
    stat_send,
    stat_recv,
    local_sem,
):
    me = lax.axis_index("sp")
    me_t = lax.axis_index("tp")
    tok = q_ref.shape[0]
    width = q_ref.shape[1]
    hd = width // heads
    feat = first.shape[1]
    cols = feat // t
    block = feat // n
    per = n // t
    half_n = n // 2

    def at_pos(p):
        p = lax.rem(p + n, n)
        back = p // half_n
        return 2 * (p + back * (n - 1 - 2 * p)) + back

    pos = me // 2 + lax.rem(me, 2) * (n - 1 - 2 * (me // 2))
    next_dev = (at_pos(pos + 1), at_pos(pos - 1))
    own_in = (kv_in, up_in, down_in)
    full = (kv, up, down)
    rows_of = (tok, block, block)

    def ring_copy(item, way, hop, piece, own=False):
        rows = rows_of[item]
        half = rows // 2
        owner = at_pos(pos - (hop - 1) if way == RIGHT else pos + (hop - 1))
        dst = full[item].at[aligned(owner * rows + piece * half, half)]
        src = own_in[item].at[aligned(piece * half, half)] if own else dst
        return pltpu.make_async_remote_copy(
            src_ref=src,
            dst_ref=dst,
            send_sem=ring_send.at[item, way, hop, piece],
            recv_sem=ring_recv.at[item, way, hop, piece],
            device_id={"sp": next_dev[way]},
            device_id_type=MESH,
        )

    def ring_landed(item, way, hop, piece):
        rows = rows_of[item]
        half = rows // 2
        owner = at_pos(pos - hop if way == RIGHT else pos + hop)
        dst = full[item].at[aligned(owner * rows + piece * half, half)]
        return pltpu.make_async_remote_copy(
            src_ref=dst,
            dst_ref=dst,
            send_sem=ring_send.at[item, way, hop, piece],
            recv_sem=ring_recv.at[item, way, hop, piece],
            device_id={"sp": next_dev[way]},
            device_id_type=MESH,
        )

    def start_own(item):
        ring_copy(item, RIGHT, 1, 0, own=True).start()
        ring_copy(item, LEFT, 1, 1, own=True).start()
        ring_copy(item, RIGHT, 1, 1, own=True).start()
        ring_copy(item, LEFT, 1, 0, own=True).start()

    def event(item, e, hop=None, second=None):
        static = isinstance(e, int)
        hop = 1 + e // 2
        second = e % 2 if static else lax.rem(e, 2)
        ring_landed(item, RIGHT, hop, second).wait_recv()

        def forward_right():
            ring_copy(item, RIGHT, hop + 1, second).start()

        def forward_left():
            ring_copy(item, LEFT, hop + 1, 1 - second).start()

        def start_next():
            if item < DOWN:
                start_own(item + 1)

        def guarded(cond, fn):
            if static:
                if cond:
                    fn()
            else:
                pl.when(cond)(fn)

        guarded(e < n - 3, forward_right)
        ring_landed(item, LEFT, hop, 1 - second).wait_recv()
        guarded(e < n - 3, forward_left)
        guarded(e == n - 4, start_next)

    def drain_sends(item):
        def one(e, _):
            hop = 1 + e // 2
            second = lax.rem(e, 2)
            ring_copy(item, RIGHT, hop, second).wait_send()
            ring_copy(item, LEFT, hop, 1 - second).wait_send()
            return 0

        lax.fori_loop(0, n - 1, one, 0)

    def peer_t(d):
        return lax.rem(me_t + d, t)

    def tp_copy(src, dst_of, sends, recvs, d):
        return pltpu.make_async_remote_copy(
            src_ref=src,
            dst_ref=dst_of(me_t),
            send_sem=sends.at[d],
            recv_sem=recvs.at[d],
            device_id={"tp": peer_t(d)},
            device_id_type=MESH,
        )

    def tp_landed(dst_of, sends, recvs, d):
        dst = dst_of(lax.rem(me_t + t - d, t))
        return pltpu.make_async_remote_copy(
            src_ref=dst,
            dst_ref=dst,
            send_sem=sends.at[d],
            recv_sem=recvs.at[d],
            device_id={"tp": peer_t(d)},
            device_id_type=MESH,
        )

    def br_copy(d, landed=False):
        owner = lax.rem(me + n - d, n) if landed else me
        return pltpu.make_async_remote_copy(
            src_ref=br.at[owner] if landed else br_in,
            dst_ref=br.at[owner],
            send_sem=br_send.at[d],
            recv_sem=br_recv.at[d],
            device_id={"sp": lax.rem(me + d, n)},
            device_id_type=MESH,
        )

    barrier = pltpu.get_barrier_semaphore()

    def greet(d, _):
        pl.semaphore_signal(
            barrier, inc=1, device_id={"sp": lax.rem(me + d, n)}, device_id_type=MESH
        )
        return 0

    lax.fori_loop(1, n, greet, 0)
    for d in range(1, t):
        pl.semaphore_signal(barrier, inc=1, device_id={"tp": peer_t(d)}, device_id_type=MESH)

    res_at = lambda g: res.at[g]
    ow_at = lambda g: ow.at[g]
    att_at = lambda g: att_all.at[g]

    locals_ = [
        pltpu.make_async_copy(kv_in, kv.at[aligned(me * tok, tok)], local_sem.at[0]),
        pltpu.make_async_copy(up_in, up.at[aligned(me * block, block)], local_sem.at[1]),
        pltpu.make_async_copy(down_in, down.at[aligned(me * block, block)], local_sem.at[2]),
        pltpu.make_async_copy(br_in, br.at[me], local_sem.at[3]),
        pltpu.make_async_copy(res_in, res.at[me_t], local_sem.at[4]),
        pltpu.make_async_copy(ow_in, ow.at[me_t], local_sem.at[5]),
    ]
    pl.semaphore_wait(barrier, n - 1 + t - 1)
    start_own(KV)

    def send_breaks(d, _):
        br_copy(d).start()
        return 0

    lax.fori_loop(1, n, send_breaks, 0)
    for c in locals_:
        c.start()
    for d in range(1, t):
        tp_copy(ow_in, ow_at, ow_send, ow_recv, d).start()
    for d in range(1, t):
        tp_copy(res_in, res_at, res_send, res_recv, d).start()

    key_row = lax.broadcasted_iota(jnp.int32, (tok, tok), 0)
    key_col = lax.broadcasted_iota(jnp.int32, (tok, tok), 1)
    lower[...] = jnp.where(key_row > key_col, 1.0, 0.0).astype(BF16)
    later_sum[...] = jnp.zeros_like(later_sum)
    totals[...] = jnp.zeros_like(totals)

    def kv_event(e, _):
        event(KV, e)
        return 0

    lax.fori_loop(0, n - 2, kv_event, 0)

    def last_event(item):
        ring_landed(item, RIGHT, half_n, 0).wait_recv()
        ring_landed(item, LEFT, half_n, 1).wait_recv()

    last_event(KV)

    def wait_breaks(d, _):
        br_copy(d, landed=True).wait_recv()
        return 0

    lax.fori_loop(1, n, wait_breaks, 0)
    for c in locals_:
        c.wait()

    scale = hd ** (-0.5)
    tile = 128

    def attend_block(j):
        b = me - j
        for h in range(heads):
            def rows(i, _):
                at = aligned(i * tile, tile)
                keys = kv[aligned(b * tok, tok), pl.ds(h * hd, hd)]
                vals = kv[aligned(b * tok, tok), pl.ds(width + h * hd, hd)]
                z = lax.dot_general(
                    q_ref[at, pl.ds(h * hd, hd)],
                    keys,
                    (((1,), (1,)), ((), ())),
                    preferred_element_type=F32,
                )
                z = z * scale + br[b, pl.ds(h, 1), :]
                soft = jnp.log(1.0 + jnp.exp(-jnp.abs(z)))
                log_break = jnp.minimum(z, 0.0) - soft
                r = lax.broadcasted_iota(jnp.int32, (tile, tok), 0) + i * tile + j * tok
                strict = lax.broadcasted_iota(jnp.int32, (tile, tok), 1) < r
                log_keep = jnp.where(strict, log_break - z, 0.0)
                high = log_keep.astype(BF16)
                low = (log_keep - high.astype(F32)).astype(BF16)
                tri = lower[...]
                later = jnp.dot(high, tri, preferred_element_type=F32) + jnp.dot(
                    low, tri, preferred_element_type=F32
                )
                before = later_sum[h, at, :]
                w = jnp.exp(log_break + later + before[:, 0:1])
                w = jnp.where(strict, w, 0.0).astype(BF16)
                totals[at, pl.ds(h * hd, hd)] += jnp.dot(w, vals, preferred_element_type=F32)
                later_sum[h, at, :] = before + jnp.sum(log_keep, axis=1, keepdims=True)
                return 0

            lax.fori_loop(0, tok // tile, rows, 0)

    def attend_step(j, _):
        @pl.when(j <= me)
        def _():
            attend_block(j)

        @pl.when(j < n - 2)
        def _():
            event(UP, j)

        return 0

    lax.fori_loop(0, n, attend_step, 0)

    own_att = att_all.at[me_t]
    own_att[...] = totals[...].astype(BF16)
    for d in range(1, t):
        tp_copy(own_att, att_at, att_send, att_recv, d).start()
    last_event(UP)
    for d in range(1, t):
        tp_landed(ow_at, ow_send, ow_recv, d).wait_recv()
        tp_landed(res_at, res_send, res_recv, d).wait_recv()
    for d in range(1, t):
        tp_landed(att_at, att_send, att_recv, d).wait_recv()

    big = 256

    def mix_rows(i, _):
        at = aligned(i * big, big)
        for c in range(t):
            lanes = pl.ds(c * cols, cols)
            acc = ALPHA * res[c, at, :].astype(F32)
            mixed = jnp.zeros((big, cols), F32)
            for g in range(t):
                mixed = mixed + jnp.dot(
                    att_all[g, at, :], ow[g, :, lanes], preferred_element_type=F32
                ).astype(BF16).astype(F32)
            pre[at, lanes] = acc + mixed
        return 0

    lax.fori_loop(0, tok // big, mix_rows, 0)
    event(DOWN, 0)

    small = 64

    def norm_rows(i, _):
        at = aligned(i * small, small)
        x = pre[at, :]
        center = jnp.sum(x, axis=1, keepdims=True) / feat
        x = x - center
        spread = jnp.sum(x * x, axis=1, keepdims=True) / feat
        first[at, :] = (x * lax.rsqrt(spread + EPSILON) * g1_ref[...] + b1_ref[...]).astype(BF16)
        return 0

    lax.fori_loop(0, tok // small, norm_rows, 0)

    hidden = up.shape[1]
    strip = 256

    def up_cols(i, _):
        lanes = aligned(i * strip, strip)
        a = jnp.dot(first[...], up[:, lanes], preferred_element_type=F32)
        a = jnp.maximum(a, 0.0)
        activated[:, lanes] = (a * a).astype(BF16)
        return 0

    event(DOWN, 1)
    lax.fori_loop(0, hidden // strip, up_cols, 0)

    def mix_copy(s):
        k = lax.rem(s, per)
        owner = s // per
        return owner, pltpu.make_async_remote_copy(
            src_ref=part.at[s],
            dst_ref=mix.at[me_t, k],
            send_sem=mix_send.at[s],
            recv_sem=mix_recv.at[me_t, k],
            device_id={"tp": owner},
            device_id_type=MESH,
        )

    def down_block(s):
        y = lax.dot_general(
            activated[...],
            down[aligned(s * block, block), :],
            (((1,), (1,)), ((), ())),
            preferred_element_type=F32,
        ).astype(BF16)
        owner, copy = mix_copy(s)

        @pl.when(owner == me_t)
        def _():
            mix[me_t, lax.rem(s, per)] = y

        @pl.when(owner != me_t)
        def _():
            part[s] = y
            copy.start()

    down_block(me)

    def down_step(h, _):
        @pl.when(h > 1)
        def _():
            event(DOWN, 2 * h - 2)
            event(DOWN, 2 * h - 1)

        def side(w, _):
            down_block(at_pos(pos + (2 * w - 1) * h))
            return 0

        lax.fori_loop(0, 2, side, 0)
        return 0

    lax.fori_loop(1, half_n, down_step, 0)
    last_event(DOWN)
    down_block(at_pos(pos + half_n))

    def mix_wait(s, _):
        owner, copy = mix_copy(s)

        @pl.when(owner != me_t)
        def _():
            copy.wait_send()

        return 0

    for d in range(1, t):
        g = lax.rem(me_t + t - d, t)
        for k in range(per):
            dst = mix.at[g, k]
            pltpu.make_async_remote_copy(
                src_ref=dst,
                dst_ref=dst,
                send_sem=mix_send.at[0],
                recv_sem=mix_recv.at[g, k],
                device_id={"tp": peer_t(d)},
                device_id_type=MESH,
            ).wait_recv()

    def second_pre(i, _):
        at = aligned(i * 128, 128)
        sums = jnp.zeros((128, 1), F32)
        squares = jnp.zeros((128, 1), F32)
        x = ALPHA * first[at, aligned(me_t * cols, cols)].astype(F32)
        pieces = []
        for k in range(per):
            v = mix[0, k, at, :].astype(F32)
            for g in range(1, t):
                v = v + mix[g, k, at, :].astype(F32)
            pieces.append(v)
        x = x + (jnp.concatenate(pieces, axis=1) if per > 1 else pieces[0])
        pre[at, pl.ds(0, cols)] = x
        sums = jnp.sum(x, axis=1, keepdims=True)
        squares = jnp.sum(x * x, axis=1, keepdims=True)
        lane = lax.broadcasted_iota(jnp.int32, (128, 128), 1)
        s = jnp.where(lane == 0, sums, jnp.where(lane == 1, squares, 0.0))
        stat[me_t, :, at] = s.T[0:8, :]
        return 0

    for i in range(tok // 128):
        second_pre(i, 0)
    stat_at = lambda g: stat.at[g]
    for d in range(1, t):
        tp_copy(stat.at[me_t], stat_at, stat_send, stat_recv, d).start()

    lax.fori_loop(0, n, mix_wait, 0)
    for item in (KV, UP, DOWN):
        drain_sends(item)

    def br_done(d, _):
        br_copy(d).wait_send()
        return 0

    lax.fori_loop(1, n, br_done, 0)
    for d in range(1, t):
        tp_copy(ow_in, ow_at, ow_send, ow_recv, d).wait_send()
        tp_copy(res_in, res_at, res_send, res_recv, d).wait_send()
        tp_copy(own_att, att_at, att_send, att_recv, d).wait_send()
    for d in range(1, t):
        tp_landed(stat_at, stat_send, stat_recv, d).wait_recv()

    for i in range(tok // 128):
        at = pl.ds(i * 128, 128)
        s = stat[0, :, at]
        for g in range(1, t):
            s = s + stat[g, :, at]
        s = jnp.concatenate([s, jnp.zeros((120, 128), F32)], axis=0).T
        center = s[:, 0:1] / feat
        spread = s[:, 1:2] / feat - center * center
        x = pre[at, pl.ds(0, cols)]
        x = (x - center) * lax.rsqrt(spread + EPSILON)
        out_ref[at, :] = (x * g2_ref[me_t] + b2_ref[me_t]).astype(BF16)
    for d in range(1, t):
        tp_copy(stat.at[me_t], stat_at, stat_send, stat_recv, d).wait_send()


GROUP = 4


def flip(a, r):
    bit = 1
    out = a
    while bit <= r:
        if r & bit:
            out = out + bit - 2 * bit * lax.rem(a // bit, 2)
        bit *= 2
    return out


def remote(src, dst, send, recv, **where):
    return pltpu.make_async_remote_copy(
        src_ref=src,
        dst_ref=dst,
        send_sem=send,
        recv_sem=recv,
        device_id=where,
        device_id_type=MESH,
    )


def grouped_kernel(
    n,
    t,
    q_in,
    k_in,
    v_in,
    br_in,
    res_in,
    ow_in,
    g1_ref,
    b1_ref,
    up_in,
    down_in,
    g2_ref,
    b2_ref,
    out_ref,
    kvb,
    qb,
    br,
    later_sum,
    totals,
    att_own,
    att_all,
    tri_ref,
    ow,
    res,
    pre,
    first,
    up,
    down,
    act,
    pair_out,
    pair_in,
    summed,
    near_in,
    held,
    side_out,
    side_in,
    cross_out,
    cross_in,
    mixed_ref,
    stat,
    kv_send,
    kv_recv,
    kx_send,
    kx_recv,
    br_send,
    br_recv,
    ow_send,
    ow_recv,
    res_send,
    res_recv,
    att_send,
    att_recv,
    w_send,
    w_recv,
    t1_send,
    t1_recv,
    t2_send,
    t2_recv,
    t3_send,
    t3_recv,
    pair_send,
    pair_recv,
    near_send,
    near_recv,
    side_send,
    side_recv,
    cross_send,
    cross_recv,
    stat_send,
    stat_recv,
    local_sem,
    go_sem,
    pair_sem,
):
    s = lax.axis_index("sp")
    q = lax.axis_index("tp")
    y = lax.rem(s, 2)
    z = s // 2
    levels = n // 2
    m = lax.rem(s, GROUP)
    group = s // GROUP
    x = q // 2
    c = lax.rem(q, 2)
    tok, width = q_in.shape
    hd = width // 2
    feat = ow.shape[2]
    cols = feat // t
    half_feat = feat // 2
    block = up_in.shape[0]
    sub = up_in.shape[1] // GROUP
    part = tok // 2
    half_n = n // 2
    sibling = flip(q, 1)
    across = flip(q, 2)

    barrier = pltpu.get_barrier_semaphore()
    for r in range(1, n):
        pl.semaphore_signal(barrier, inc=1, device_id={"sp": flip(s, r)}, device_id_type=MESH)
    for r in range(1, t):
        pl.semaphore_signal(barrier, inc=1, device_id={"tp": flip(q, r)}, device_id_type=MESH)
        pl.semaphore_signal(
            barrier, inc=1, device_id={"sp": flip(s, 1), "tp": flip(q, r)}, device_id_type=MESH
        )

    def lanes_of(i, size):
        return aligned(i * size, size)

    own_copies = [
        pltpu.make_async_copy(
            k_in.at[:, lanes_of(y, hd)], kvb.at[s, :, pl.ds(0, hd)], local_sem.at[0]
        ),
        pltpu.make_async_copy(
            v_in.at[:, lanes_of(y, hd)], kvb.at[s, :, pl.ds(hd, hd)], local_sem.at[1]
        ),
        pltpu.make_async_copy(q_in.at[:, lanes_of(y, hd)], qb.at[y], local_sem.at[2]),
    ]
    other_copies = [
        pltpu.make_async_copy(br_in, br.at[s], local_sem.at[3]),
        pltpu.make_async_copy(res_in.at[lanes_of(c, part)], res.at[q], local_sem.at[4]),
        pltpu.make_async_copy(ow_in, ow.at[q], local_sem.at[5]),
        pltpu.make_async_copy(
            up_in.at[:, lanes_of(m, sub)], up.at[lanes_of(s, block)], local_sem.at[6]
        ),
        pltpu.make_async_copy(
            down_in.at[:, lanes_of(m, sub)], down.at[lanes_of(s, block)], local_sem.at[7]
        ),
    ]
    for cp in own_copies:
        cp.start()

    ps = flip(s, 1)
    py = 1 - y

    def exchange(landed=False):
        own = ps if landed else s
        row = y if landed else py
        mine = py if landed else y
        return [
            remote(
                kvb.at[own, :, pl.ds(0, hd)] if landed else k_in.at[:, lanes_of(row, hd)],
                kvb.at[own, :, pl.ds(0, hd)],
                kx_send.at[0],
                kx_recv.at[0],
                sp=ps,
            ),
            remote(
                kvb.at[own, :, pl.ds(hd, hd)] if landed else v_in.at[:, lanes_of(row, hd)],
                kvb.at[own, :, pl.ds(hd, hd)],
                kx_send.at[1],
                kx_recv.at[1],
                sp=ps,
            ),
            remote(
                qb.at[mine] if landed else q_in.at[:, lanes_of(row, hd)],
                qb.at[mine],
                kx_send.at[2],
                kx_recv.at[2],
                sp=ps,
            ),
        ]

    def relay(slot):
        return remote(kvb.at[slot], kvb.at[slot], kv_send.at[slot], kv_recv.at[slot], sp=s + 2)

    def relay_landed(slot):
        return remote(kvb.at[slot], kvb.at[slot], kv_send.at[slot], kv_recv.at[slot], sp=s)

    def br_copy(r, landed=False):
        owner = flip(s, r) if landed else s
        return remote(
            br.at[owner] if landed else br_in,
            br.at[owner],
            br_send.at[r],
            br_recv.at[owner],
            sp=flip(s, r),
        )

    def ow_copy(r, landed=False):
        owner = flip(q, r) if landed else q
        return remote(
            ow.at[owner] if landed else ow_in,
            ow.at[owner],
            ow_send.at[r],
            ow_recv.at[r],
            tp=flip(q, r),
        )

    def ow_pass(landed=False):
        ref = ow.at[flip(q, 3) if landed else across]
        return remote(ref, ref, ow_send.at[3], ow_recv.at[3], tp=sibling)

    def res_copy(r, landed=False):
        to = flip(q, r)
        owner = to if landed else q
        return remote(
            res.at[owner] if landed else res_in.at[lanes_of(lax.rem(to, 2), part)],
            res.at[owner],
            res_send.at[r],
            res_recv.at[r],
            tp=to,
        )

    mats_in = (up_in, down_in)
    mats = (up, down)

    def w_copy(mat, r, landed=False):
        to = flip(s, r)
        owner = to if landed else s
        dst = mats[mat].at[lanes_of(owner, block)]
        return remote(
            dst if landed else mats_in[mat].at[:, lanes_of(lax.rem(to, GROUP), sub)],
            dst,
            w_send.at[mat, r],
            w_recv.at[mat, r],
            sp=to,
        )

    def climbs(r):
        return lax.rem(s // (half_n if r >= half_n else 2), 2) == 0

    def send_mat(mat, rs, upward):
        for r in rs:

            def go(r=r):
                w_copy(mat, r).start()

            if r < 2:
                go()
            else:
                pl.when(climbs(r) if upward else jnp.logical_not(climbs(r)))(go)

    def send_up(mat, skip=()):
        far_level = [r for r in range(half_n, n) if (r // 2) % 2 and r not in skip]
        same_level = [r for r in range(half_n, n) if not (r // 2) % 2 and r not in skip]

        @pl.when(group == 0)
        def _():
            @pl.when(lax.rem(z, 2) == 0)
            def _():
                for r in same_level + far_level:
                    w_copy(mat, r).start()

            @pl.when(lax.rem(z, 2) == 1)
            def _():
                for r in far_level + same_level:
                    w_copy(mat, r).start()

    straight = [r for r in range(n - 1, 0, -1) if r % 2 == 0]
    turning = [r for r in range(n - 1, 0, -1) if r % 2]

    pl.semaphore_wait(barrier, n - 1 + 2 * (t - 1))
    for cp in exchange():
        cp.start()
    for r in range(1, n):
        br_copy(r).start()
    for cp in other_copies:
        cp.start()
    for cp in own_copies:
        cp.wait()

    @pl.when(z < levels - 1)
    def _():
        relay(s).start()

    for r in range(1, t):
        res_copy(r).start()
    for r in (1, 2):
        ow_copy(r).start()
    send_mat(0, straight, False)

    inner = lax.rem(z, 2) != group
    far_straight = [r for r in straight if r >= half_n]

    key_row = lax.broadcasted_iota(jnp.int32, tri_ref.shape, 0)
    key_col = lax.broadcasted_iota(jnp.int32, tri_ref.shape, 1)
    tri_ref[...] = jnp.where(key_row > key_col, 1.0, 0.0).astype(BF16)
    later_sum[...] = jnp.zeros_like(later_sum)
    totals[...] = jnp.zeros_like(totals)

    for cp in other_copies:
        cp.wait()

    def br_landed(slot):
        remote(br.at[slot], br.at[slot], br_send.at[0], br_recv.at[slot], sp=s).wait_recv()

    scale = hd ** (-0.5)
    tile = 512
    span = tri_ref.shape[0]

    def attend(slot, qy, masked):
        def rows(i, _):
            at = aligned(i * tile, tile)
            z_ = lax.dot_general(
                qb[qy, at, :],
                kvb[slot, :, pl.ds(0, hd)],
                (((1,), (1,)), ((), ())),
                preferred_element_type=F32,
            )
            z_ = z_ * scale + br[slot, pl.ds(y, 1), :]
            soft = jnp.log(1.0 + jnp.exp(-jnp.abs(z_)))
            log_break = jnp.minimum(z_, 0.0) - soft
            keep = log_break - z_
            if masked:
                r = lax.broadcasted_iota(jnp.int32, (tile, tok), 0) + i * tile
                strict = lax.broadcasted_iota(jnp.int32, (tile, tok), 1) < r
                keep = jnp.where(strict, keep, 0.0)
            high = keep.astype(BF16)
            low = (keep - high.astype(F32)).astype(BF16)
            tri = tri_ref[...]
            run = later_sum[qy, at, :][:, 0:1]
            pieces = []
            for b in range(tok // span - 1, -1, -1):
                sl = slice(b * span, (b + 1) * span)
                later = jnp.dot(high[:, sl], tri, preferred_element_type=F32) + jnp.dot(
                    low[:, sl], tri, preferred_element_type=F32
                )
                pieces.append(later + run)
                run = run + jnp.sum(keep[:, sl], axis=1, keepdims=True)
            w = jnp.exp(log_break + jnp.concatenate(pieces[::-1], axis=1))
            if masked:
                w = jnp.where(strict, w, 0.0)
            totals[qy, at, :] += jnp.dot(
                w.astype(BF16), kvb[slot, :, pl.ds(hd, hd)], preferred_element_type=F32
            )
            later_sum[qy, at, :] = jnp.broadcast_to(run, (tile, 128))
            return 0

        lax.fori_loop(0, tok // tile, rows, 0)

    attend(s, y, True)
    for cp in exchange(landed=True):
        cp.wait_recv()

    @pl.when(z < levels - 1)
    def _():
        relay(ps).start()

    br_landed(ps)
    send_mat(0, turning, False)
    attend(ps, py, True)

    def fetch(slot):
        @pl.when(slot >= 0)
        def _():
            relay_landed(slot).wait_recv()
            br_landed(slot)

            @pl.when(z < levels - 1)
            def _():
                relay(slot).start()

    ahead = jnp.where(z < levels - 1, 2, 0)

    @pl.when(z < levels - 1)
    def _():
        fetch(2 * z - 1)

    attend(2 * z, 1, False)

    @pl.when(z < levels - 1)
    def _():
        fetch(2 * z - 2)

    def attend_step(k, _):
        slot = 2 * z + 1 - k
        fetch(slot - ahead)

        @pl.when(slot >= 0)
        def _():
            def one(qy, _):
                attend(slot, qy, False)
                return 0

            lax.fori_loop(0, 2, one, 0)

        return 0

    lax.fori_loop(2, n, attend_step, 0)

    @pl.when(z < levels - 1)
    def _():
        def drain(slot, _):
            relay(slot).wait_send()
            return 0

        lax.fori_loop(0, 2 * z + 2, drain, 0)
        pl.semaphore_signal(pair_sem, inc=1, device_id={"tp": sibling}, device_id_type=MESH)
        pl.semaphore_wait(pair_sem, 1)

    send_mat(0, (2, 3), True)

    @pl.when(z == 1)
    def _():
        pl.semaphore_signal(go_sem, inc=1, device_id={"sp": s - 2}, device_id_type=MESH)

    @pl.when(z == 0)
    def _():
        pl.semaphore_wait(go_sem, 1)

    send_up(0)

    @pl.when(inner)
    def _():
        send_mat(1, far_straight[:1], False)
        send_mat(1, far_straight[:1], True)

    ow_copy(2, landed=True).wait_recv()
    ow_pass().start()

    att_own[...] = totals[...].astype(BF16)
    att_list = [(dy, r) for dy in range(2) for r in range(t) if dy or r]

    def att_copy(i, landed=False):
        dy, r = att_list[i]
        ty = flip(y, 1) if dy else y
        tq = flip(q, r)
        sp = ps if dy else s
        if landed:
            dst = att_all.at[tq, :, lanes_of(ty, hd)]
            return remote(dst, dst, att_send.at[i], att_recv.at[i], sp=sp, tp=tq)
        return remote(
            att_own.at[ty, lanes_of(lax.rem(tq, 2), part)],
            att_all.at[q, :, lanes_of(y, hd)],
            att_send.at[i],
            att_recv.at[i],
            sp=sp,
            tp=tq,
        )

    for i in range(len(att_list)):
        att_copy(i).start()
    att_all[q, :, lanes_of(y, hd)] = att_own[y, lanes_of(c, part), :]
    ow_copy(1, landed=True).wait_recv()
    ow_pass(landed=True).wait_recv()
    for r in range(1, t):
        res_copy(r, landed=True).wait_recv()
    for i in range(len(att_list)):
        att_copy(i, landed=True).wait_recv()

    for cc in range(t):
        lanes = pl.ds(cc * cols, cols)
        mixed = jnp.zeros((part, cols), F32)
        for g in range(t):
            mixed = mixed + jnp.dot(
                att_all[g], ow[g, :, lanes], preferred_element_type=F32
            ).astype(BF16).astype(F32)
        pre[:, lanes] = ALPHA * res[cc].astype(F32) + mixed

    small = 64

    def norm_rows(i, _):
        at = aligned(i * small, small)
        v = pre[at, :]
        center = jnp.sum(v, axis=1, keepdims=True) / feat
        v = v - center
        spread = jnp.sum(v * v, axis=1, keepdims=True) / feat
        v = (v * lax.rsqrt(spread + EPSILON) * g1_ref[...] + b1_ref[...]).astype(BF16)
        first[m, c, 0, at, :] = v[:, :half_feat]
        first[m, c, 1, at, :] = v[:, half_feat:]
        return 0

    lax.fori_loop(0, part // small, norm_rows, 0)

    def member(r):
        return flip(m, r)

    def group_dev(r):
        return flip(s, r)

    quarter = part // 2

    def t1_copy(r, e, landed=False):
        owner = member(r) if landed else (member(2) if r == 3 else m)
        ref = first.at[owner, c, x, pl.ds(e * quarter, quarter)]
        return remote(
            ref, ref, t1_send.at[r, e], t1_recv.at[r, e], sp=group_dev(1 if r == 3 else r)
        )

    def t2_copy(r, e, landed=False):
        ref = first.at[member(r), c, 1 - x if landed else x, pl.ds(e * quarter, quarter)]
        return remote(ref, ref, t2_send.at[r, e], t2_recv.at[r, e], tp=across)

    def t3_copy(r, h, e, landed=False):
        xh = x if h == 0 else 1 - x
        ref = first.at[member(r), 1 - c if landed else c, xh, pl.ds(e * quarter, quarter)]
        return remote(ref, ref, t3_send.at[r, h, e], t3_recv.at[r, h, e], tp=sibling)

    for e in range(2):
        for r in (2, 1):
            t1_copy(r, e).start()
    for e in range(2):
        for h in range(2):
            t3_copy(0, h, e).start()
    send_mat(1, [r for r in straight if r < half_n], False)

    @pl.when(jnp.logical_not(inner))
    def _():
        send_mat(1, far_straight[1:], False)
        send_mat(1, far_straight[1:], True)

    def up_block(mm):
        def one(i, _):
            ch = i // 2
            lanes = aligned(lax.rem(i, 2) * (sub // 2), sub // 2)
            a = jnp.dot(
                first[mm, ch, 0], up[pl.ds(0, half_feat), lanes], preferred_element_type=F32
            ) + jnp.dot(
                first[mm, ch, 1],
                up[pl.ds(half_feat, half_feat), lanes],
                preferred_element_type=F32,
            )
            a = jnp.maximum(a, 0.0)
            act[aligned(mm * tok + ch * part, part), lanes] = (a * a).astype(BF16)
            return 0

        lax.fori_loop(0, 4, one, 0)

    def pass_on(steps):
        for r, e in steps:
            t1_copy(r, e, landed=True).wait_recv()
            if r == 2:
                t1_copy(3, e).start()
            t2_copy(r, e).start()
            t3_copy(r, 0, e).start()

    pass_on(((1, 0), (2, 0), (1, 1), (2, 1)))
    send_mat(1, [r for r in turning if r > 1], False)
    send_mat(1, (1,), False)
    send_mat(1, (2, 3), True)
    send_up(1, far_straight)

    @pl.when(inner)
    def _():
        send_mat(1, far_straight[1:], False)
        send_mat(1, far_straight[1:], True)

    @pl.when(jnp.logical_not(inner))
    def _():
        send_mat(1, far_straight[:1], False)
        send_mat(1, far_straight[:1], True)

    for e in range(2):
        for h in range(2):
            t3_copy(0, h, e, landed=True).wait_recv()
    for r in range(1, n):
        w_copy(0, r, landed=True).wait_recv()
    up_block(m)
    pass_on(((3, 0), (3, 1)))
    for r in (1, 2, 3):
        for e in range(2):
            t2_copy(r, e, landed=True).wait_recv()
            t3_copy(r, 1, e).start()
        for e in range(2):
            for h in range(2):
                t3_copy(r, h, e, landed=True).wait_recv()
        up_block(member(r))

    def piece(mm, tq):
        return lax.dot_general(
            act[aligned(mm * tok, tok), :],
            down[lanes_of(tq, cols), :],
            (((1,), (1,)), ((), ())),
            preferred_element_type=F32,
        )

    def pair_copy(p, mm):
        return remote(
            pair_out.at[p, mm],
            pair_in.at[p, mm],
            pair_send.at[p, mm],
            pair_recv.at[p, mm],
            tp=sibling,
        )

    def near_copy(p, h, r):
        return remote(
            summed.at[p, h, member(r)],
            near_in.at[p, h, r],
            near_send.at[p, h, r],
            near_recv.at[p, h, r],
            sp=group_dev(r if r < 3 else lead(h)),
        )

    def lead(h):
        return 1 if h else 2

    def near_on(p, h):
        near_copy(p, h, 3).wait_recv()
        rest = 3 - lead(h)
        both = summed[p, h, member(rest)].astype(F32) + near_in[p, h, 3].astype(F32)
        summed[p, h, member(rest)] = both.astype(BF16)
        near_copy(p, h, rest).start()

    def side_copy(mm):
        return remote(side_out.at[mm], side_in.at[mm], side_send.at[mm], side_recv.at[mm], tp=across)

    def cross_copy():
        return remote(cross_out, cross_in, cross_send.at[0], cross_recv.at[0], tp=across)

    member_order = (3, 1, 2, 0)

    def reduce_phase(p):
        xp = group if p == 0 else 1 - group
        far = range(half_n, n) if p else range(1, half_n)
        for r in far:
            w_copy(1, r, landed=True).wait_recv()
        for r in member_order:
            mm = member(r)
            pair_out[p, mm] = piece(mm, 2 * xp + 1 - c).astype(BF16)
            pair_copy(p, mm).start()
        for r in member_order:
            mm = member(r)
            pair_copy(p, mm).wait_recv()
            both = piece(mm, 2 * xp + c) + pair_in[p, mm].astype(F32)
            summed[p, 1, mm] = both[:, block:].astype(BF16)
            if r % 2:
                near_copy(p, 1, r).start()
            v = both[:, :block]

            @pl.when(xp == x)
            def _():
                held[p, mm] = v

            @pl.when(xp != x)
            def _():
                side_out[mm] = v.astype(BF16)
                side_copy(mm).start()

    def side_phase(p, rs):
        xp = group if p == 0 else 1 - group

        @pl.when(xp == x)
        def _():
            for r in rs:
                mm = member(r)
                side_copy(mm).wait_recv()
                if r:
                    summed[p, 0, mm] = (held[p, mm] + side_in[mm].astype(F32)).astype(BF16)
                if r in (3, lead(0)):
                    near_copy(p, 0, r).start()
            if 0 in rs:
                near_on(p, 0)

    def gather_phase(p, mine):
        xp = group if p == 0 else 1 - group

        def total(at):
            v = summed[p, 1, m, at, :].astype(F32)
            for r in (1, 2):
                v = v + near_in[p, 1, r, at, :].astype(F32)
            return v

        @pl.when(xp == x if mine else xp != x)
        def _():
            for r in (1, 2):
                near_copy(p, 1, r).wait_recv()
                if mine:
                    near_copy(p, 0, r).wait_recv()

            def rows(i, _):
                at = aligned(i * 64, 64)
                if mine:
                    mixed_ref[at, pl.ds(block, block)] = total(at)
                    v = held[p, m, at, :] + side_in[m, at, :].astype(F32)
                    for r in (1, 2):
                        v = v + near_in[p, 0, r, at, :].astype(F32)
                    mixed_ref[at, pl.ds(0, block)] = v
                else:
                    cross_out[at, :] = total(at).astype(BF16)
                return 0

            lax.fori_loop(0, tok // 64, rows, 0)
            if not mine:
                cross_copy().start()

    reduce_phase(0)
    reduce_phase(1)
    near_on(0, 1)
    for p in range(2):
        side_phase(p, member_order[:2])
    gather_phase(0, False)
    near_on(1, 1)
    for p in range(2):
        side_phase(p, member_order[2:])
    gather_phase(1, False)
    for p in range(2):
        gather_phase(p, True)
    cross_copy().wait_recv()

    row_tile = 128
    for i in range(tok // row_tile):
        at = pl.ds(i * row_tile, row_tile)
        ch = i // (part // row_tile)
        inner = pl.ds((i % (part // row_tile)) * row_tile, row_tile)
        v = ALPHA * first[m, ch, x, inner, lanes_of(c, cols)].astype(F32)
        v = v + jnp.concatenate(
            [
                mixed_ref[at, pl.ds(0, block)],
                mixed_ref[at, pl.ds(block, block)] + cross_in[at, :].astype(F32),
            ],
            axis=1,
        )
        mixed_ref[at, :] = v
        sums = jnp.sum(v, axis=1, keepdims=True)
        squares = jnp.sum(v * v, axis=1, keepdims=True)
        lane = lax.broadcasted_iota(jnp.int32, (row_tile, 128), 1)
        st = jnp.where(lane == 0, sums, jnp.where(lane == 1, squares, 0.0))
        stat[q, :, at] = st.T[0:8, :]

    def stat_copy(r, landed=False):
        owner = flip(q, r) if landed else q
        return remote(
            stat.at[owner], stat.at[owner], stat_send.at[r], stat_recv.at[r], tp=flip(q, r)
        )

    for r in range(1, t):
        stat_copy(r).start()

    for cp in exchange():
        cp.wait_send()
    def br_rest(slot, _):
        br_landed(slot)
        return 0

    lax.fori_loop(2 * z + 2, n, br_rest, 0)
    for r in range(1, n):
        br_copy(r).wait_send()
        w_copy(0, r).wait_send()
        w_copy(1, r).wait_send()
    for r in (1, 2):
        ow_copy(r).wait_send()
    ow_pass().wait_send()
    for r in range(1, t):
        res_copy(r).wait_send()
    for i in range(len(att_list)):
        att_copy(i).wait_send()
    for r in range(1, GROUP):
        for e in range(2):
            t1_copy(r, e).wait_send()
            t2_copy(r, e).wait_send()
        for p in range(2):
            near_copy(p, 1, r).wait_send()
        near_copy(jnp.where(group == x, 0, 1), 0, r).wait_send()
    for r in range(GROUP):
        for h in range(2):
            for e in range(2):
                t3_copy(r, h, e).wait_send()
        for p in range(2):
            pair_copy(p, r).wait_send()
        side_copy(r).wait_send()
    cross_copy().wait_send()

    for r in range(1, t):
        stat_copy(r, landed=True).wait_recv()
    for i in range(tok // row_tile):
        at = pl.ds(i * row_tile, row_tile)
        st = stat[0, :, at]
        for g in range(1, t):
            st = st + stat[g, :, at]
        st = jnp.concatenate([st, jnp.zeros((120, row_tile), F32)], axis=0).T
        center = st[:, 0:1] / feat
        spread = st[:, 1:2] / feat - center * center
        v = (mixed_ref[at, :] - center) * lax.rsqrt(spread + EPSILON)
        out_ref[at, :] = (v * g2_ref[q] + b2_ref[q]).astype(BF16)
    for r in range(1, t):
        stat_copy(r).wait_send()


def grouped_call(n, t, args):
    (
        queries,
        keys,
        values,
        breaks,
        residual_in,
        out_weight,
        first_gain,
        first_shift,
        up_weight,
        down_weight,
        second_gain,
        second_shift,
    ) = args
    tok, width = queries.shape
    heads = breaks.shape[1]
    hd = width // heads
    feat = out_weight.shape[1]
    cols = residual_in.shape[1]
    sub = up_weight.shape[1] // GROUP
    part = tok // 2
    br = jnp.pad(breaks.astype(F32).T, ((0, 8 - heads), (0, 0)))
    any_ = pl.BlockSpec(memory_space=pl.ANY)
    vmem = pl.BlockSpec(memory_space=pltpu.VMEM)
    dma = pltpu.SemaphoreType.DMA
    v = pltpu.VMEM
    return pl.pallas_call(
        functools.partial(grouped_kernel, n, t),
        out_shape=jax.ShapeDtypeStruct((tok, cols), BF16),
        in_specs=[any_] * 6 + [vmem, vmem, any_, any_, vmem, vmem],
        out_specs=vmem,
        scratch_shapes=[
            v((n, tok, 2 * hd), BF16),
            v((2, tok, hd), BF16),
            v((n, 8, tok), F32),
            v((2, tok, 128), F32),
            v((2, tok, hd), F32),
            v((2, tok, hd), BF16),
            v((t, part, width), BF16),
            v((256, 256), BF16),
            v((t, width, feat), BF16),
            v((t, part, cols), BF16),
            v((part, feat), F32),
            v((GROUP, 2, 2, part, feat // 2), BF16),
            v((feat, sub), BF16),
            v((feat, sub), BF16),
            v((GROUP * tok, sub), BF16),
            v((2, GROUP, tok, cols), BF16),
            v((2, GROUP, tok, cols), BF16),
            v((2, 2, GROUP, tok, cols // 2), BF16),
            v((2, 2, GROUP, tok, cols // 2), BF16),
            v((2, GROUP, tok, cols // 2), F32),
            v((GROUP, tok, cols // 2), BF16),
            v((GROUP, tok, cols // 2), BF16),
            v((tok, cols // 2), BF16),
            v((tok, cols // 2), BF16),
            v((tok, cols), F32),
            v((t, 8, tok), F32),
            dma((n,)),
            dma((n,)),
            dma((3,)),
            dma((3,)),
            dma((n,)),
            dma((n,)),
            dma((t,)),
            dma((t,)),
            dma((t,)),
            dma((t,)),
            dma((2 * t - 1,)),
            dma((2 * t - 1,)),
            dma((2, n)),
            dma((2, n)),
            dma((GROUP, 2)),
            dma((GROUP, 2)),
            dma((GROUP, 2)),
            dma((GROUP, 2)),
            dma((GROUP, 2, 2)),
            dma((GROUP, 2, 2)),
            dma((2, GROUP)),
            dma((2, GROUP)),
            dma((2, 2, GROUP)),
            dma((2, 2, GROUP)),
            dma((GROUP,)),
            dma((GROUP,)),
            dma((1,)),
            dma((1,)),
            dma((t,)),
            dma((t,)),
            dma((8,)),
            pltpu.SemaphoreType.REGULAR,
            pltpu.SemaphoreType.REGULAR,
        ],
        compiler_params=pltpu.CompilerParams(
            collective_id=0, has_side_effects=True, vmem_limit_bytes=62 * 1024 * 1024
        ),
    )(
        queries,
        keys,
        values,
        br,
        residual_in,
        out_weight,
        first_gain.reshape(1, feat),
        first_shift.reshape(1, feat),
        up_weight,
        down_weight,
        second_gain.reshape(t, 1, cols),
        second_shift.reshape(t, 1, cols),
    )


def solution(mesh):
    n, t = mesh.shape["sp"], mesh.shape["tp"]

    def body(
        queries,
        keys,
        values,
        breaks,
        residual_in,
        out_weight,
        first_gain,
        first_shift,
        up_weight,
        down_weight,
        second_gain,
        second_shift,
    ):
        tok, width = queries.shape
        heads = breaks.shape[1]
        if heads == 2 and t == 4 and n == 2 * GROUP:
            return grouped_call(
                n,
                t,
                (
                    queries,
                    keys,
                    values,
                    breaks,
                    residual_in,
                    out_weight,
                    first_gain,
                    first_shift,
                    up_weight,
                    down_weight,
                    second_gain,
                    second_shift,
                ),
            )
        feat = out_weight.shape[1]
        cols = residual_in.shape[1]
        hidden = up_weight.shape[1]
        block = up_weight.shape[0]
        per = n // t
        kv = jnp.concatenate([keys, values], axis=1)
        br = jnp.pad(breaks.astype(F32).T, ((0, 8 - heads), (0, 0)))
        any_ = pl.BlockSpec(memory_space=pl.ANY)
        vmem = pl.BlockSpec(memory_space=pltpu.VMEM)
        dma = pltpu.SemaphoreType.DMA
        ring = dma((3, 2, n // 2 + 1, 2))
        return pl.pallas_call(
            functools.partial(layer_kernel, n, t, heads),
            out_shape=jax.ShapeDtypeStruct((tok, cols), BF16),
            in_specs=[vmem, any_, any_, any_, any_, vmem, vmem, any_, any_, vmem, vmem],
            out_specs=vmem,
            scratch_shapes=[
                pltpu.VMEM((n * tok, 2 * width), BF16),
                pltpu.VMEM((feat, hidden), BF16),
                pltpu.VMEM((feat, hidden), BF16),
                pltpu.VMEM((n, 8, tok), F32),
                pltpu.VMEM((t, width, feat), BF16),
                pltpu.VMEM((t, tok, cols), BF16),
                pltpu.VMEM((heads, tok, 128), F32),
                pltpu.VMEM((tok, width), F32),
                pltpu.VMEM((t, tok, width), BF16),
                pltpu.VMEM((tok, tok), BF16),
                pltpu.VMEM((tok, feat), F32),
                pltpu.VMEM((tok, feat), BF16),
                pltpu.VMEM((tok, hidden), BF16),
                pltpu.VMEM((n, tok, block), BF16),
                pltpu.VMEM((t, per, tok, block), BF16),
                pltpu.VMEM((t, 8, tok), F32),
                ring,
                ring,
                dma((n,)),
                dma((n,)),
                dma((t,)),
                dma((t,)),
                dma((t,)),
                dma((t,)),
                dma((t,)),
                dma((t,)),
                dma((n,)),
                dma((t, per)),
                dma((t,)),
                dma((t,)),
                dma((6,)),
            ],
            compiler_params=pltpu.CompilerParams(
                collective_id=0, has_side_effects=True, vmem_limit_bytes=62 * 1024 * 1024
            ),
        )(
            queries,
            kv,
            br,
            residual_in,
            out_weight,
            first_gain.reshape(1, feat),
            first_shift.reshape(1, feat),
            up_weight,
            down_weight,
            second_gain.reshape(t, 1, cols),
            second_shift.reshape(t, 1, cols),
        )

    return jax.shard_map(
        body,
        mesh=mesh,
        in_specs=(
            P("sp", "tp"),
            P("sp", "tp"),
            P("sp", "tp"),
            P("sp", "tp"),
            P("sp", "tp"),
            P("tp", None),
            P(),
            P(),
            P("sp", "tp"),
            P("sp", "tp"),
            P(),
            P(),
        ),
        out_specs=P("sp", "tp"),
        check_vma=False,
    )
```
